512 devices in a mesh: fs: 64 (over z, y), tp: 8 (over x, core).
Axes of the slice: x: 4, y: 8, z: 8, core: 2. Of those that a mesh axis runs over, the one named last changes fastest.
Arguments:
- normed: bfloat16 [65536, 2048], P('fs'), may hold values from -6 to 6
- key_cot: bfloat16 [65536, 1024], P('fs', 'tp'), may hold values from -130 to 130
- value_cot: bfloat16 [65536, 2048], P('fs', 'tp'), may hold values from -130 to 130
- basis: bfloat16 [2048, 256], P('fs'), may hold values from -3.535534 to 3.535534
- master_key: float32 [2048, 1024], P('fs', 'tp'), may hold values from -3 to 3
- master_value: float32 [2048, 2048], P('fs', 'tp'), may hold values from -3 to 3
- first_key: float32 [256, 1024], P('fs', 'tp'), may hold values from -3 to 3
- second_key: float32 [256, 1024], P('fs', 'tp'), may hold values from 0.05 to 2
- first_value: float32 [256, 2048], P('fs', 'tp'), may hold values from -3 to 3
- second_value: float32 [256, 2048], P('fs', 'tp'), may hold values from 0.05 to 2
Outputs:
- step_key: float32 [2048, 1024], P('fs', 'tp')
- step_value: float32 [2048, 2048], P('fs', 'tp')
- new_master_key: float32 [2048, 1024], P('fs', 'tp')
- new_master_value: float32 [2048, 2048], P('fs', 'tp')
- copy_key: bfloat16 [2048, 1024], P(None, 'tp')
- copy_value: bfloat16 [2048, 2048], P(None, 'tp')
- new_first_key: float32 [256, 1024], P('fs', 'tp')
- new_second_key: float32 [256, 1024], P('fs', 'tp')
- new_first_value: float32 [256, 2048], P('fs', 'tp')
- new_second_value: float32 [256, 2048], P('fs', 'tp')
The draws below stay inside these ranges and needn't reach their ends.
All inputs are finite; a program needn't handle non-finite values.
Results may differ from the reference program's by a relative error of at most 0.0055.
Values may be sent and summed in bfloat16 or wider, within the bound.
No kernel may reach another device: no remote copies, remote signals or barrier semaphores. Data moves between devices by JAX's collectives and lax.ppermute only.
A program may use at most 64 MiB of HBM per device.

```python
import math
import jax
import jax.numpy as jnp
from jax import lax

D = 2048
DK = 1024
DV = 2048
R = 256
TOKENS = 65536


def column_scaled(key, height, width):
    keys = jax.random.split(key, 2)
    ramp = jnp.arange(width, dtype=jnp.float32) / max(width - 1, 1)
    jitter = jnp.exp(jax.random.uniform(keys[1], (width,), jnp.float32, math.log(0.7), math.log(1.4)))
    scales = 10.0 ** ramp * jitter
    base_values = jnp.clip(jax.random.normal(keys[0], (height, width), jnp.float32), -6.0, 6.0)
    return base_values * scales[None, :]


def draw_basis(key, part):
    values = column_scaled(jax.random.fold_in(key, 11), D, R) * D ** (-0.5)
    return values.astype(jnp.bfloat16)


def draw_key_cot(key, part):
    return column_scaled(jax.random.fold_in(key, 12), TOKENS, DK).astype(jnp.bfloat16)


def draw_value_cot(key, part):
    return column_scaled(jax.random.fold_in(key, 13), TOKENS, DV).astype(jnp.bfloat16)


def shard_levels(stream_key, dims, cuts, low, largest):
    factor_of, own = 1.0, jax.random.fold_in(stream_key, 6)
    for dim, blocks in cuts:
        steps = jnp.exp(jax.random.uniform(jax.random.fold_in(own, dim), (blocks,), jnp.float32, low / len(cuts), largest / len(cuts)))
        factor_of = factor_of * jnp.repeat(steps, dims[dim] // blocks).reshape([-1 if axis == dim else 1 for axis in range(len(dims))])
    return factor_of


def noise(stream_key, extent, deviation, limit, cuts=(), kind=jnp.bfloat16):
    gain = shard_levels(stream_key, extent, cuts, -0.22, 0.18) if cuts else 1.0
    drawn = jax.random.normal(stream_key, extent, jnp.float32) * deviation * gain
    return jnp.minimum(jnp.maximum(drawn, -limit), limit).astype(kind)


def setup_inputs(seed: int = 0) -> dict:
    arg_keys = jax.random.split(jax.random.key(seed), 11)
    return {
        "normed": noise(arg_keys[0], (TOKENS, D), 1.0, 6.0, ((0, 64),)),
        "key_cot": draw_key_cot(jax.random.fold_in(arg_keys[10], 71), 0),
        "value_cot": draw_value_cot(jax.random.fold_in(arg_keys[10], 71), 0),
        "basis": draw_basis(jax.random.fold_in(arg_keys[10], 71), 0),
        "master_key": noise(arg_keys[4], (D, DK), 0.5, 3.0, ((0, 64), (1, 8)), jnp.float32),
        "master_value": noise(arg_keys[5], (D, DV), 0.5, 3.0, ((0, 64), (1, 8)), jnp.float32),
        "first_key": noise(arg_keys[6], (R, DK), 0.5, 3.0, ((0, 64), (1, 8)), jnp.float32),
        "second_key": jnp.clip(jnp.exp(math.log(2.0) - 3.6888794 * jax.random.uniform(arg_keys[7], (R, DK), jnp.float32) ** shard_levels(arg_keys[7], (R, DK), ((0, 64), (1, 8)), -0.2, 0.2)), 0.05, 2.0),
        "first_value": noise(arg_keys[8], (R, DV), 0.5, 3.0, ((0, 64), (1, 8)), jnp.float32),
        "second_value": jnp.clip(jnp.exp(math.log(2.0) - 3.6888794 * jax.random.uniform(arg_keys[9], (R, DV), jnp.float32) ** shard_levels(arg_keys[9], (R, DV), ((0, 64), (1, 8)), -0.2, 0.2)), 0.05, 2.0),
    }


learn_rate = 0.05
beta_first = 0.9
beta_second = 0.9
epsilon = 1e-08
norm_eps = 1e-06

def moment_update(low_grad, grad_scale, first_moment, second_moment, basis):
    scaled = low_grad * grad_scale
    new_first = beta_first * first_moment + (1.0 - beta_first) * scaled
    new_second = beta_second * second_moment + (1.0 - beta_second) * scaled * scaled
    direction = (new_first / (jnp.sqrt(new_second) + epsilon)).astype(jnp.bfloat16)
    update_step = jnp.dot(basis, direction, preferred_element_type=jnp.float32)
    return (update_step, new_first, new_second)

def reference(normed, key_cot, value_cot, basis, master_key, master_value, first_key, second_key, first_value, second_value):
    grad_key = jnp.dot(normed.T, key_cot, preferred_element_type=jnp.float32)
    grad_value = jnp.dot(normed.T, value_cot, preferred_element_type=jnp.float32)
    basis_wide = basis.astype(jnp.float32).T
    low_key = jnp.dot(basis_wide, grad_key, precision=lax.Precision.HIGHEST, preferred_element_type=jnp.float32)
    low_value = jnp.dot(basis_wide, grad_value, precision=lax.Precision.HIGHEST, preferred_element_type=jnp.float32)
    squares = jnp.sum(low_key * low_key) + jnp.sum(low_value * low_value)
    root_mean = jnp.sqrt(squares / (R * (DK + DV)) + norm_eps)
    grad_scale = 1.0 / root_mean
    step_key, new_first_key, new_second_key = moment_update(low_key, grad_scale, first_key, second_key, basis)
    step_value, new_first_value, new_second_value = moment_update(low_value, grad_scale, first_value, second_value, basis)
    new_master_key = master_key - learn_rate * step_key
    new_master_value = master_value - learn_rate * step_value
    return (step_key, step_value, new_master_key, new_master_value, new_master_key.astype(jnp.bfloat16), new_master_value.astype(jnp.bfloat16), new_first_key, new_second_key, new_first_value, new_second_value)
```

```python
import jax
import jax.numpy as jnp
from jax import lax
from jax.sharding import Mesh
from jax.sharding import PartitionSpec as P

DK = 1024
DV = 2048
R = 256
FS = ("fs_0", "fs_1")
TP = ("tp_0", "tp_1")

learn_rate = 0.05
beta_first = 0.9
beta_second = 0.9
epsilon = 1e-08
norm_eps = 1e-06


f32 = jnp.float32
bf16 = jnp.bfloat16


def to_everyone(array, axis):
    copies = jnp.broadcast_to(array, (lax.axis_size(axis), *array.shape))
    return lax.all_to_all(copies, axis, split_axis=0, concat_axis=0, tiled=True)


def dot0(a, b):
    return lax.dot_general(a, b, (((0,), (0,)), ((), ())), preferred_element_type=f32)


def dot(a, b):
    return jnp.dot(a, b, preferred_element_type=f32)


def moments(low, scale, first, second):
    scaled = low * scale
    new_first = beta_first * first + (1.0 - beta_first) * scaled
    new_second = beta_second * second + (1.0 - beta_second) * scaled * scaled
    return new_first, new_second


def on_device(normed, key_cot, value_cot, basis, mk, mv, fk, sk, fv, sv):
    kc = key_cot.shape[1]
    rows = basis.shape[0]
    own = fk.shape[0]
    n_fs = lax.axis_size(FS)
    half = R // 2
    core = lax.axis_index("tp_1")

    master = jnp.concatenate([mk, mv], axis=1)
    first = jnp.concatenate([fk, fv], axis=1)
    second = jnp.concatenate([sk, sv], axis=1)
    pack = jnp.concatenate([master, first, second], axis=0).astype(bf16)
    pack, basis = lax.optimization_barrier((pack, basis))
    gathered = lax.all_gather(pack, FS, axis=0, tiled=False)

    my_half = lax.dynamic_slice(basis, (0, core * half), (rows, half))
    basis_mine = to_everyone(my_half, FS).reshape(n_fs * rows, half)
    basis_other = lax.ppermute(basis_mine, "tp_1", [(0, 1), (1, 0)])

    cot = jnp.concatenate([key_cot, value_cot], axis=1)
    grad = dot0(normed, cot)
    hi = grad.astype(bf16)
    lo = (grad - hi.astype(f32)).astype(bf16)
    low_mine = dot0(basis_mine, hi) + dot0(basis_mine, lo)
    low_other = dot0(basis_other, hi) + dot0(basis_other, lo)
    parts = jnp.where(
        core == 0,
        jnp.concatenate([low_mine, low_other], axis=0),
        jnp.concatenate([low_other, low_mine], axis=0),
    )
    tiles = lax.all_to_all(parts.reshape(n_fs, own, -1), FS, 0, 0, tiled=True)
    own_low = jnp.sum(tiles, axis=0)

    all_low = to_everyone(own_low.astype(bf16), FS).astype(f32)
    local = jnp.sum(all_low * all_low)
    squares = jnp.sum(to_everyone(jnp.full((1, 128), local, f32), TP)[:, 0, 0])
    scale = 1.0 / jnp.sqrt(squares / (R * (DK + DV)) + norm_eps)

    new_first, new_second = moments(own_low, scale, first, second)
    all_first = gathered[:, rows : rows + own].astype(f32)
    all_second = gathered[:, rows + own :].astype(f32)
    nf, ns = moments(all_low, scale, all_first, all_second)
    direction = (nf / (jnp.sqrt(ns) + epsilon)).astype(bf16).reshape(R, -1)

    step = dot(basis, direction)
    new_master = master - learn_rate * step
    dir_mine = lax.dynamic_slice(direction, (core * half, 0), (half, direction.shape[1]))
    dir_other = lax.dynamic_slice(direction, ((1 - core) * half, 0), (half, direction.shape[1]))
    all_step = dot(basis_mine, dir_mine) + dot(basis_other, dir_other)
    all_master = gathered[:, :rows].reshape(n_fs * rows, -1).astype(f32)
    copy = (all_master - learn_rate * all_step).astype(bf16)
    return (
        step[:, :kc],
        step[:, kc:],
        new_master[:, :kc],
        new_master[:, kc:],
        copy[:, :kc],
        copy[:, kc:],
        new_first[:, :kc],
        new_second[:, :kc],
        new_first[:, kc:],
        new_second[:, kc:],
    )


def solution(mesh):
    torus = Mesh(mesh.devices.reshape(8, 8, 4, 2), ("fs_0", "fs_1", "tp_0", "tp_1"))
    split = P(FS, TP)
    in_specs = (P(FS, None), split, split, P(FS, None)) + (split,) * 6
    out_specs = (split,) * 4 + (P(None, TP),) * 2 + (split,) * 4
    return jax.shard_map(
        on_device, mesh=torus, in_specs=in_specs, out_specs=out_specs, check_vma=False
    )
```

```python
import jax
import jax.numpy as jnp
from jax import lax
from jax.experimental import pallas as pl
from jax.experimental.pallas import tpu as pltpu
from jax.sharding import Mesh
from jax.sharding import PartitionSpec as P

DK = 1024
DV = 2048
R = 256
FS = ("fs_0", "fs_1")
TP = ("tp_0", "tp_1")

learn_rate = 0.05
beta_first = 0.9
beta_second = 0.9
epsilon = 1e-08
norm_eps = 1e-06


f32 = jnp.float32
bf16 = jnp.bfloat16
VMEM = pl.BlockSpec(memory_space=pltpu.VMEM)
SMEM = pl.BlockSpec(memory_space=pltpu.SMEM)
ANY = pl.BlockSpec(memory_space=pl.ANY)
HBM = pl.BlockSpec(memory_space=pltpu.HBM)


def shape(dims, dtype):
    return jax.ShapeDtypeStruct(dims, dtype)


def cost(flops, moved):
    return pl.CostEstimate(flops=flops, bytes_accessed=moved, transcendentals=0)


def limit(mib):
    return pltpu.CompilerParams(vmem_limit_bytes=mib * 1024 * 1024)


def dot(a, b):
    return jnp.dot(a, b, preferred_element_type=f32)


def pack_kernel(core, mk, mv, fk, fv, sk, sv, basis, pack, copies):
    kc = mk.shape[1]
    rows, half = copies.shape[1], copies.shape[2]
    pack[:rows, :kc] = mk[...].astype(bf16)
    pack[:rows, kc:] = mv[...].astype(bf16)
    keys = jnp.concatenate([fk[...], sk[...]], axis=0)
    values = jnp.concatenate([fv[...], sv[...]], axis=0)
    pack[rows:, :kc] = keys.astype(bf16)
    pack[rows:, kc:] = values.astype(bf16)
    mine = jnp.where(core[0] == 0, basis[:, :half].astype(f32), basis[:, half:].astype(f32))
    copies[...] = jnp.broadcast_to(mine.astype(bf16)[None], copies.shape)


def project_kernel(hi, lo, basis, out):
    b = basis[...]
    out[...] = (dot(hi[...], b) + dot(lo[...], b)).T


def project_both_kernel(core, hi, lo, basis, mine, out):
    half = mine.shape[0]
    b = basis[...]
    at = pl.multiple_of(core[0] * half, half)
    other = pl.multiple_of((1 - core[0]) * half, half)
    out[pl.ds(at, half), :] = mine[...]
    out[pl.ds(other, half), :] = (dot(hi[...], b) + dot(lo[...], b)).T


def squares_kernel(low, out):
    x = low[...].astype(f32)
    out[...] = jnp.broadcast_to(jnp.sum(x * x, keepdims=True)[None], out.shape)


def moments(low, scale, first, second):
    scaled = low * scale
    new_first = beta_first * first + (1.0 - beta_first) * scaled
    new_second = beta_second * second + (1.0 - beta_second) * scaled * scaled
    return new_first, new_second


def final_kernel(
    core, squares, low, own_low, fk, fv, sk, sv, mk, mv, basis, mine, other, gathered,
    step_k, step_v, new_k, new_v, copy_k, copy_v, nf_k, ns_k, nf_v, ns_v,
    mom, masters, b_mine, b_other, direction, out_k, out_v, in_sem, master_sem, out_sem,
):
    n_fs, per, _ = mom.shape
    rows = mk.shape[0]
    kc = mk.shape[1]
    half = b_mine.shape[1]
    chunks = master_sem.shape[0]
    group = n_fs // chunks
    loads = [
        pltpu.make_async_copy(gathered.at[:, pl.ds(rows, per), :], mom, in_sem.at[0]),
        pltpu.make_async_copy(mine, b_mine, in_sem.at[1]),
        pltpu.make_async_copy(other, b_other, in_sem.at[2]),
    ]
    for k in range(chunks):
        at = pl.ds(k * group, group)
        loads.append(
            pltpu.make_async_copy(
                gathered.at[at, pl.ds(0, rows), :], masters.at[at], master_sem.at[k]
            )
        )
    for load in loads:
        load.start()

    total = jnp.sum(squares[...], axis=0)[:1, :1]
    scale = 1.0 / jnp.sqrt(total / (R * (DK + DV)) + norm_eps)

    nf, ns = moments(own_low[:, :kc], scale, fk[...], sk[...])
    nf_k[...] = nf
    ns_k[...] = ns
    nf, ns = moments(own_low[:, kc:], scale, fv[...], sv[...])
    nf_v[...] = nf
    ns_v[...] = ns

    own = per // 2
    i = lax.broadcasted_iota(jnp.int32, (n_fs * own, n_fs * per), 0)
    j = lax.broadcasted_iota(jnp.int32, (n_fs * own, n_fs * per), 1)
    at_first = (i // own) * per + i % own
    pick_first = jnp.where(j == at_first, 1.0, 0.0).astype(bf16)
    pick_second = jnp.where(j == at_first + own, 1.0, 0.0).astype(bf16)
    loads[0].wait()
    both = mom[...].reshape(n_fs * per, mom.shape[2])
    all_first = dot(pick_first, both)
    all_second = dot(pick_second, both)
    nf, ns = moments(low[...].astype(f32), scale, all_first, all_second)
    direction[...] = (nf / (jnp.sqrt(ns) + epsilon)).astype(bf16)

    step = dot(basis[...], direction[...])
    step_k[...] = step[:, :kc]
    step_v[...] = step[:, kc:]
    new_k[...] = mk[...] - learn_rate * step[:, :kc]
    new_v[...] = mv[...] - learn_rate * step[:, kc:]

    at = pl.multiple_of(core[0] * half, half)
    at_other = pl.multiple_of((1 - core[0]) * half, half)
    ordered = jnp.concatenate(
        [direction[pl.ds(at, half), :], direction[pl.ds(at_other, half), :]], axis=0
    )
    loads[1].wait()
    loads[2].wait()
    stores = []
    for k in range(chunks):
        size = group * rows
        at = pl.ds(k * size, size)
        both = jnp.concatenate([b_mine[at, :], b_other[at, :]], axis=1)
        step = dot(both, ordered)
        loads[3 + k].wait()
        master = masters[pl.ds(k * group, group)].astype(f32).reshape(size, -1)
        copy = (master - learn_rate * step).astype(bf16)
        out_k[at, :] = copy[:, :kc]
        out_v[at, :] = copy[:, kc:]
        stores.append(pltpu.make_async_copy(out_k.at[at], copy_k.at[at], out_sem.at[0, k]))
        stores.append(pltpu.make_async_copy(out_v.at[at], copy_v.at[at], out_sem.at[1, k]))
        stores[-2].start()
        stores[-1].start()
    for store in stores:
        store.wait()


def to_everyone(array, axis):
    copies = jnp.broadcast_to(array, (lax.axis_size(axis), *array.shape))
    return lax.all_to_all(copies, axis, split_axis=0, concat_axis=0, tiled=True)


def on_device(normed, key_cot, value_cot, basis, mk, mv, fk, sk, fv, sv):
    kc = key_cot.shape[1]
    cols = kc + value_cot.shape[1]
    rows = basis.shape[0]
    d = normed.shape[1]
    own = fk.shape[0]
    n_fs = lax.axis_size(FS)
    n_tp = lax.axis_size(TP)
    half = R // 2
    core = lax.axis_index("tp_1").astype(jnp.int32).reshape(1)

    pack, copies = pl.pallas_call(
        pack_kernel,
        out_shape=(shape((rows + 2 * own, cols), bf16), shape((n_fs, rows, half), bf16)),
        in_specs=[SMEM] + [VMEM] * 7,
        out_specs=(VMEM, VMEM),
        compiler_params=limit(62),
        name="pack",
    )(core, mk, mv, fk, fv, sk, sv, basis)
    gathered = lax.all_gather(pack, FS, axis=0, tiled=False)
    basis_mine = lax.all_to_all(copies, FS, 0, 0, tiled=True).reshape(d, half)
    cot = jnp.concatenate([key_cot, value_cot], axis=1)
    grad = lax.dot_general(cot, normed, (((0,), (0,)), ((), ())), preferred_element_type=f32)
    hi = grad.astype(bf16)
    lo = (grad - hi.astype(f32)).astype(bf16)
    basis_mine, hi, lo = lax.optimization_barrier((basis_mine, hi, lo))
    basis_other = lax.ppermute(basis_mine, "tp_1", [(0, 1), (1, 0)])

    project_cost = cost(4 * d * half * cols, 4 * d * cols + 2 * d * half)
    low_mine = pl.pallas_call(
        project_kernel,
        out_shape=shape((half, cols), f32),
        in_specs=[VMEM] * 3,
        out_specs=VMEM,
        cost_estimate=project_cost,
        compiler_params=limit(12),
        name="project_mine",
    )(hi, lo, basis_mine)
    parts = pl.pallas_call(
        project_both_kernel,
        out_shape=shape((R, cols), f32),
        in_specs=[SMEM] + [VMEM] * 4,
        out_specs=VMEM,
        cost_estimate=project_cost,
        compiler_params=limit(12),
        name="project_other",
    )(core, hi, lo, basis_other, low_mine)
    tiles = lax.all_to_all(parts.reshape(n_fs, own, cols), FS, 0, 0, tiled=True)
    own_low = jnp.sum(tiles, axis=0)

    all_low = to_everyone(own_low.astype(bf16), FS).reshape(R, cols)
    local = pl.pallas_call(
        squares_kernel,
        out_shape=shape((n_tp, 8, 128), f32),
        in_specs=[VMEM],
        out_specs=VMEM,
        compiler_params=limit(4),
        name="squares",
    )(all_low)
    squares = lax.all_to_all(local, TP, 0, 0, tiled=True)

    chunks = 8
    vc = cols - kc
    return pl.pallas_call(
        final_kernel,
        out_shape=(
            shape((rows, kc), f32),
            shape((rows, vc), f32),
            shape((rows, kc), f32),
            shape((rows, vc), f32),
            shape((d, kc), bf16),
            shape((d, vc), bf16),
            shape((own, kc), f32),
            shape((own, kc), f32),
            shape((own, vc), f32),
            shape((own, vc), f32),
        ),
        in_specs=[SMEM] + [VMEM] * 10 + [ANY] * 2 + [HBM],
        out_specs=(VMEM,) * 4 + (HBM,) * 2 + (VMEM,) * 4,
        scratch_shapes=[
            pltpu.VMEM((n_fs, 2 * own, cols), bf16),
            pltpu.VMEM((n_fs, rows, cols), bf16),
            pltpu.VMEM((d, half), bf16),
            pltpu.VMEM((d, half), bf16),
            pltpu.VMEM((R, cols), bf16),
            pltpu.VMEM((d, kc), bf16),
            pltpu.VMEM((d, vc), bf16),
            pltpu.SemaphoreType.DMA((3,)),
            pltpu.SemaphoreType.DMA((chunks,)),
            pltpu.SemaphoreType.DMA((2, chunks)),
        ],
        compiler_params=limit(60),
        name="update",
    )(core, squares, all_low, own_low, fk, fv, sk, sv, mk, mv, basis, basis_mine, basis_other, gathered)


def solution(mesh):
    torus = Mesh(mesh.devices.reshape(8, 8, 4, 2), ("fs_0", "fs_1", "tp_0", "tp_1"))
    split = P(FS, TP)
    in_specs = (P(FS, None), split, split, P(FS, None)) + (split,) * 6
    out_specs = (split,) * 4 + (P(None, TP),) * 2 + (split,) * 4
    return jax.shard_map(
        on_device, mesh=torus, in_specs=in_specs, out_specs=out_specs, check_vma=False
    )
```

```python
import jax
import jax.numpy as jnp
from jax import lax
from jax.experimental import pallas as pl
from jax.experimental.pallas import tpu as pltpu
from jax.sharding import Mesh
from jax.sharding import PartitionSpec as P

DK = 1024
DV = 2048
R = 256
FS = ("fs_0", "fs_1", "fs_2")
RING = ("fs_0", "fs_1")
TP = ("tp_0", "tp_1")

learn_rate = 0.05
beta_first = 0.9
beta_second = 0.9
epsilon = 1e-08
norm_eps = 1e-06


f32 = jnp.float32
bf16 = jnp.bfloat16
VMEM = pl.BlockSpec(memory_space=pltpu.VMEM)
SMEM = pl.BlockSpec(memory_space=pltpu.SMEM)
ANY = pl.BlockSpec(memory_space=pl.ANY)
HBM = pl.BlockSpec(memory_space=pltpu.HBM)


def shape(dims, dtype):
    return jax.ShapeDtypeStruct(dims, dtype)


def cost(flops, moved):
    return pl.CostEstimate(flops=flops, bytes_accessed=moved, transcendentals=0)


def in_hbm(array):
    return pltpu.with_memory_space_constraint(array, pltpu.HBM)


def limit(mib):
    return pltpu.CompilerParams(vmem_limit_bytes=mib * 1024 * 1024)


def dot(a, b):
    return jnp.dot(a, b, preferred_element_type=f32)


def pack_kernel(core, mk, mv, fk, fv, sk, sv, basis, pack, copies):
    kc = mk.shape[1]
    rows, half = copies.shape[1], copies.shape[2]
    pack[:rows, :kc] = mk[...].astype(bf16)
    pack[:rows, kc:] = mv[...].astype(bf16)
    keys = jnp.concatenate([fk[...], sk[...]], axis=0)
    values = jnp.concatenate([fv[...], sv[...]], axis=0)
    pack[rows:, :kc] = keys.astype(bf16)
    pack[rows:, kc:] = values.astype(bf16)
    mine = jnp.where(core[0] == 0, basis[:, :half].astype(f32), basis[:, half:].astype(f32))
    copies[...] = jnp.broadcast_to(mine.astype(bf16)[None], copies.shape)


def project_kernel(hi, lo, basis, out):
    b = basis[...]
    out[...] = (dot(hi[...], b) + dot(lo[...], b)).T


def project_both_kernel(core, hi, lo, basis, mine, out, kept, sem):
    half = mine.shape[0]
    keep = pltpu.make_async_copy(basis, kept, sem)
    keep.start()
    b = basis[...]
    at = pl.multiple_of(core[0] * half, half)
    other = pl.multiple_of((1 - core[0]) * half, half)
    out[pl.ds(at, half), :] = mine[...]
    out[pl.ds(other, half), :] = (dot(hi[...], b) + dot(lo[...], b)).T
    keep.wait()


def squares_kernel(low, out):
    x = low[...].astype(f32)
    out[...] = jnp.broadcast_to(jnp.sum(x * x, keepdims=True)[None], out.shape)


def moments(low, scale, first, second):
    scaled = low * scale
    new_first = beta_first * first + (1.0 - beta_first) * scaled
    new_second = beta_second * second + (1.0 - beta_second) * scaled * scaled
    return new_first, new_second


def pair_kernel(odd, mine, other, out):
    out[odd[0]] = mine[...]
    out[1 - odd[0]] = other[...]


def prep_kernel(gathered, first, second, mom, sem):
    n_fs, per, _ = mom.shape
    rows = gathered.shape[1] - per
    load = pltpu.make_async_copy(gathered.at[:, pl.ds(rows, per), :], mom, sem)
    load.start()
    own = per // 2
    i = lax.broadcasted_iota(jnp.int32, (n_fs * own, n_fs * per), 0)
    j = lax.broadcasted_iota(jnp.int32, (n_fs * own, n_fs * per), 1)
    at_first = (i // own) * per + i % own
    pick_first = jnp.where(j == at_first, 1.0, 0.0).astype(bf16)
    pick_second = jnp.where(j == at_first + own, 1.0, 0.0).astype(bf16)
    load.wait()
    both = mom[...].reshape(n_fs * per, mom.shape[2])
    first[...] = dot(pick_first, both).astype(bf16)
    second[...] = dot(pick_second, both).astype(bf16)


def final_kernel(
    core, squares, low_h, all_first_h, all_second_h, own_low_h, fk_h, fv_h, sk_h, sv_h, basis_h, mk_h, mv_h,
    b_mine_h, b_other_h, gathered,
    step_k, step_v, new_k, new_v, copy_k, copy_v, nf_k, ns_k, nf_v, ns_v,
    low, all_first, all_second, own_low, fk, fv, sk, sv, basis, mk, mv, b_mine, b_other,
    masters, direction, out_k, out_v,
    step_ks, step_vs, new_ks, new_vs, nf_ks, ns_ks, nf_vs, ns_vs, in_sem, master_sem, out_sem, own_sem,
):
    n_fs = masters.shape[0]
    rows = mk.shape[0]
    kc = mk.shape[1]
    half = b_mine.shape[1]
    chunks = master_sem.shape[0]
    group = n_fs // chunks
    here = (low, all_first, all_second, own_low, fk, fv, sk, sv, basis, mk, mv, b_mine, b_other)
    there = (
        low_h, all_first_h, all_second_h, own_low_h, fk_h, fv_h, sk_h, sv_h, basis_h, mk_h, mv_h,
        b_mine_h, b_other_h,
    )
    inputs = []
    for k in range(len(here)):
        inputs.append(pltpu.make_async_copy(there[k], here[k], in_sem.at[k]))
        inputs[k].start()
    loads = []
    for k in range(chunks):
        at = pl.ds(k * group, group)
        loads.append(
            pltpu.make_async_copy(
                gathered.at[at, pl.ds(0, rows), :], masters.at[at], master_sem.at[k]
            )
        )
        loads[k].start()

    stores = []

    def store(source, target, sem):
        stores.append(pltpu.make_async_copy(source, target, sem))
        stores[-1].start()

    for item in inputs[:3]:
        item.wait()
    total = jnp.sum(squares[...], axis=0)[:1, :1]
    scale = 1.0 / jnp.sqrt(total / (R * (DK + DV)) + norm_eps)

    nf, ns = moments(low[...].astype(f32), scale, all_first[...].astype(f32), all_second[...].astype(f32))
    direction[...] = (nf / (jnp.sqrt(ns) + epsilon)).astype(bf16)

    for item in inputs[3:]:
        item.wait()
    nf_ks[...], ns_ks[...] = moments(own_low[:, :kc], scale, fk[...], sk[...])
    nf_vs[...], ns_vs[...] = moments(own_low[:, kc:], scale, fv[...], sv[...])
    step = dot(basis[...], direction[...])
    step_ks[...] = step[:, :kc]
    step_vs[...] = step[:, kc:]
    new_ks[...] = mk[...] - learn_rate * step[:, :kc]
    new_vs[...] = mv[...] - learn_rate * step[:, kc:]
    sources = (step_ks, step_vs, new_ks, new_vs, nf_ks, ns_ks, nf_vs, ns_vs)
    targets = (step_k, step_v, new_k, new_v, nf_k, ns_k, nf_v, ns_v)
    for k in range(len(sources)):
        store(sources[k], targets[k], own_sem.at[k])

    at = pl.multiple_of(core[0] * half, half)
    at_other = pl.multiple_of((1 - core[0]) * half, half)
    ordered = jnp.concatenate(
        [direction[pl.ds(at, half), :], direction[pl.ds(at_other, half), :]], axis=0
    )
    for k in range(chunks):
        size = group * rows
        at = pl.ds(k * size, size)
        both = jnp.concatenate([b_mine[at, :], b_other[at, :]], axis=1)
        step = dot(both, ordered)
        loads[k].wait()
        master = masters[pl.ds(k * group, group)].astype(f32).reshape(size, -1)
        copy = (master - learn_rate * step).astype(bf16)
        out_k[at, :] = copy[:, :kc]
        out_v[at, :] = copy[:, kc:]
        store(out_k.at[at], copy_k.at[at], out_sem.at[0, k])
        store(out_v.at[at], copy_v.at[at], out_sem.at[1, k])
    for item in stores:
        item.wait()


def to_everyone(array, axis):
    copies = jnp.broadcast_to(array, (lax.axis_size(axis), *array.shape))
    return lax.all_to_all(copies, axis, split_axis=0, concat_axis=0, tiled=True)


def on_device(normed, key_cot, value_cot, basis, mk, mv, fk, sk, fv, sv):
    kc = key_cot.shape[1]
    cols = kc + value_cot.shape[1]
    rows = basis.shape[0]
    d = normed.shape[1]
    own = fk.shape[0]
    n_fs = lax.axis_size(FS)
    n_tp = lax.axis_size(TP)
    half = R // 2
    core = lax.axis_index("tp_1").astype(jnp.int32).reshape(1)
    odd = lax.axis_index("fs_2").astype(jnp.int32).reshape(1)
    per = rows + 2 * own
    pair = [(0, 1), (1, 0)]

    pack, copies = pl.pallas_call(
        pack_kernel,
        out_shape=(shape((per, cols), bf16), shape((n_fs, rows, half), bf16)),
        in_specs=[SMEM] + [VMEM] * 7,
        out_specs=(VMEM, VMEM),
        compiler_params=limit(24),
        name="pack",
    )(core, *(in_hbm(x) for x in (mk, mv, fk, fv, sk, sv, basis)))
    other_pack = lax.ppermute(pack, "fs_2", pair)
    both_packs = pl.pallas_call(
        pair_kernel,
        out_shape=shape((2, per, cols), bf16),
        in_specs=[SMEM] + [VMEM] * 2,
        out_specs=VMEM,
        compiler_params=limit(24),
        name="pair",
    )(odd, pack, other_pack)
    gathered = lax.all_gather(both_packs.reshape(2 * per, cols), RING, axis=0, tiled=True)
    gathered = gathered.reshape(n_fs, per, cols)
    basis_mine = lax.all_to_all(copies, FS, 0, 0, tiled=True).reshape(d, half)

    cot = jnp.concatenate([key_cot, value_cot], axis=1)
    grad = lax.dot_general(cot, normed, (((0,), (0,)), ((), ())), preferred_element_type=f32)
    hi = grad.astype(bf16)
    lo = (grad - hi.astype(f32)).astype(bf16)
    basis_mine, hi, lo = lax.optimization_barrier((basis_mine, hi, lo))
    basis_other = lax.ppermute(basis_mine, "tp_1", pair)
    project_cost = cost(4 * d * half * cols, 4 * d * cols + 2 * d * half)
    low_mine = pl.pallas_call(
        project_kernel,
        out_shape=shape((half, cols), f32),
        in_specs=[VMEM] * 3,
        out_specs=VMEM,
        cost_estimate=project_cost,
        compiler_params=limit(12),
        name="project_mine",
    )(hi, lo, basis_mine)
    parts, basis_other = pl.pallas_call(
        project_both_kernel,
        out_shape=(shape((R, cols), f32), pltpu.HBM((d, half), bf16)),
        in_specs=[SMEM] + [VMEM] * 4,
        out_specs=(VMEM, HBM),
        scratch_shapes=[pltpu.SemaphoreType.DMA],
        cost_estimate=project_cost,
        compiler_params=limit(12),
        name="project_other",
    )(core, hi, lo, basis_other, low_mine)
    tiles = lax.all_to_all(parts.reshape(n_fs, own, cols), FS, 0, 0, tiled=True)
    own_low = jnp.sum(tiles, axis=0)

    all_low = to_everyone(own_low.astype(bf16), FS).reshape(R, cols)
    local = pl.pallas_call(
        squares_kernel,
        out_shape=shape((n_tp, 8, 128), f32),
        in_specs=[VMEM],
        out_specs=VMEM,
        compiler_params=limit(4),
        name="squares",
    )(all_low)
    squares = lax.all_to_all(local, TP, 0, 0, tiled=True)
    all_first, all_second = pl.pallas_call(
        prep_kernel,
        out_shape=(shape((R, cols), bf16), shape((R, cols), bf16)),
        in_specs=[ANY],
        out_specs=(VMEM, VMEM),
        scratch_shapes=[
            pltpu.VMEM((n_fs, 2 * own, cols), bf16),
            pltpu.SemaphoreType.DMA,
        ],
        cost_estimate=cost(4 * R * 2 * R * cols, 2 * n_fs * per * cols),
        compiler_params=limit(24),
        name="prep",
    )(in_hbm(gathered))

    chunks = 8
    vc = cols - kc
    small = ((rows, kc), (rows, vc)) * 2 + ((own, kc), (own, kc), (own, vc), (own, vc))
    outs = tuple(shape(dims, f32) for dims in small)
    return pl.pallas_call(
        final_kernel,
        out_shape=outs[:4] + (shape((d, kc), bf16), shape((d, vc), bf16)) + outs[4:],
        in_specs=[SMEM, VMEM] + [ANY] * 14,
        out_specs=(HBM,) * 10,
        scratch_shapes=[
            pltpu.VMEM((R, cols), bf16),
            pltpu.VMEM((R, cols), bf16),
            pltpu.VMEM((R, cols), bf16),
            pltpu.VMEM((own, cols), f32),
            pltpu.VMEM((own, kc), f32),
            pltpu.VMEM((own, vc), f32),
            pltpu.VMEM((own, kc), f32),
            pltpu.VMEM((own, vc), f32),
            pltpu.VMEM((rows, R), bf16),
            pltpu.VMEM((rows, kc), f32),
            pltpu.VMEM((rows, vc), f32),
            pltpu.VMEM((d, half), bf16),
            pltpu.VMEM((d, half), bf16),
            pltpu.VMEM((n_fs, rows, cols), bf16),
            pltpu.VMEM((R, cols), bf16),
            pltpu.VMEM((d, kc), bf16),
            pltpu.VMEM((d, vc), bf16),
        ]
        + [pltpu.VMEM(dims, f32) for dims in small]
        + [
            pltpu.SemaphoreType.DMA((13,)),
            pltpu.SemaphoreType.DMA((chunks,)),
            pltpu.SemaphoreType.DMA((2, chunks)),
            pltpu.SemaphoreType.DMA((8,)),
        ],
        compiler_params=limit(40),
        name="update",
    )(
        core, squares, all_low, all_first, all_second, own_low,
        *(in_hbm(x) for x in (fk, fv, sk, sv, basis, mk, mv, basis_mine, basis_other, gathered)),
    )


def solution(mesh):
    names = ("fs_0", "fs_1", "fs_2", "tp_0", "tp_1")
    torus = Mesh(mesh.devices.reshape(8, 4, 2, 4, 2), names)
    split = P(FS, TP)
    in_specs = (P(FS, None), split, split, P(FS, None)) + (split,) * 6
    out_specs = (split,) * 4 + (P(None, TP),) * 2 + (split,) * 4
    return jax.shard_map(
        on_device, mesh=torus, in_specs=in_specs, out_specs=out_specs, check_vma=False
    )
```

```python
import jax
import jax.numpy as jnp
from jax import lax
from jax.experimental import pallas as pl
from jax.experimental.pallas import tpu as pltpu
from jax.sharding import Mesh
from jax.sharding import PartitionSpec as P

DK = 1024
DV = 2048
R = 256
FS = ("fs_0", "fs_1", "fs_2", "fs_3")
RING = ("fs_0",)
PAIRS = ("fs_3", "fs_2", "fs_1")
TP = ("tp_0", "tp_1")

learn_rate = 0.05
beta_first = 0.9
beta_second = 0.9
epsilon = 1e-08
norm_eps = 1e-06


f32 = jnp.float32
bf16 = jnp.bfloat16
VMEM = pl.BlockSpec(memory_space=pltpu.VMEM)
SMEM = pl.BlockSpec(memory_space=pltpu.SMEM)
ANY = pl.BlockSpec(memory_space=pl.ANY)
HBM = pl.BlockSpec(memory_space=pltpu.HBM)


def shape(dims, dtype):
    return jax.ShapeDtypeStruct(dims, dtype)


def cost(flops, moved):
    return pl.CostEstimate(flops=flops, bytes_accessed=moved, transcendentals=0)


def in_hbm(array):
    return pltpu.with_memory_space_constraint(array, pltpu.HBM)


def limit(mib):
    return pltpu.CompilerParams(vmem_limit_bytes=mib * 1024 * 1024)


def dot(a, b):
    return jnp.dot(a, b, preferred_element_type=f32)


def pack_kernel(core, mk, mv, fk, fv, sk, sv, basis, pack, copies):
    kc = mk.shape[1]
    rows, half = copies.shape[1], copies.shape[2]
    pack[:rows, :kc] = mk[...].astype(bf16)
    pack[:rows, kc:] = mv[...].astype(bf16)
    keys = jnp.concatenate([fk[...], sk[...]], axis=0)
    values = jnp.concatenate([fv[...], sv[...]], axis=0)
    pack[rows:, :kc] = keys.astype(bf16)
    pack[rows:, kc:] = values.astype(bf16)
    mine = jnp.where(core[0] == 0, basis[:, :half].astype(f32), basis[:, half:].astype(f32))
    copies[...] = jnp.broadcast_to(mine.astype(bf16)[None], copies.shape)


def project_kernel(hi, lo, basis, out):
    b = basis[...]
    out[...] = (dot(hi[...], b) + dot(lo[...], b)).T


def project_both_kernel(core, hi, lo, basis, mine, out, kept, sem):
    half = mine.shape[0]
    keep = pltpu.make_async_copy(basis, kept, sem)
    keep.start()
    b = basis[...]
    at = pl.multiple_of(core[0] * half, half)
    other = pl.multiple_of((1 - core[0]) * half, half)
    out[pl.ds(at, half), :] = mine[...]
    out[pl.ds(other, half), :] = (dot(hi[...], b) + dot(lo[...], b)).T
    keep.wait()


def squares_kernel(low, out):
    x = low[...].astype(f32)
    out[...] = jnp.broadcast_to(jnp.sum(x * x, keepdims=True)[None], out.shape)


def moments(low, scale, first, second):
    scaled = low * scale
    new_first = beta_first * first + (1.0 - beta_first) * scaled
    new_second = beta_second * second + (1.0 - beta_second) * scaled * scaled
    return new_first, new_second


def pair_kernel(odd, mine, other, out):
    out[odd[0]] = mine[...]
    out[1 - odd[0]] = other[...]


def prep_kernel(gathered, first, second, mom, sem):
    n_fs, per, _ = mom.shape
    rows = gathered.shape[1] - per
    load = pltpu.make_async_copy(gathered.at[:, pl.ds(rows, per), :], mom, sem)
    load.start()
    own = per // 2
    i = lax.broadcasted_iota(jnp.int32, (n_fs * own, n_fs * per), 0)
    j = lax.broadcasted_iota(jnp.int32, (n_fs * own, n_fs * per), 1)
    at_first = (i // own) * per + i % own
    pick_first = jnp.where(j == at_first, 1.0, 0.0).astype(bf16)
    pick_second = jnp.where(j == at_first + own, 1.0, 0.0).astype(bf16)
    load.wait()
    both = mom[...].reshape(n_fs * per, mom.shape[2])
    first[...] = dot(pick_first, both).astype(bf16)
    second[...] = dot(pick_second, both).astype(bf16)


def final_kernel(
    core, squares, low_h, all_first_h, all_second_h, own_low_h, fk_h, fv_h, sk_h, sv_h, basis_h, mk_h, mv_h,
    b_mine_h, b_other_h, gathered,
    step_k, step_v, new_k, new_v, copy_k, copy_v, nf_k, ns_k, nf_v, ns_v,
    low, all_first, all_second, own_low, fk, fv, sk, sv, basis, mk, mv, b_mine, b_other,
    masters, direction, out_k, out_v,
    step_ks, step_vs, new_ks, new_vs, nf_ks, ns_ks, nf_vs, ns_vs, in_sem, master_sem, out_sem, own_sem,
):
    n_fs = masters.shape[0]
    rows = mk.shape[0]
    kc = mk.shape[1]
    half = b_mine.shape[1]
    chunks = master_sem.shape[0]
    group = n_fs // chunks
    here = (low, all_first, all_second, own_low, fk, fv, sk, sv, basis, mk, mv, b_mine, b_other)
    there = (
        low_h, all_first_h, all_second_h, own_low_h, fk_h, fv_h, sk_h, sv_h, basis_h, mk_h, mv_h,
        b_mine_h, b_other_h,
    )
    inputs = []
    for k in range(len(here)):
        inputs.append(pltpu.make_async_copy(there[k], here[k], in_sem.at[k]))
        inputs[k].start()
    loads = []
    for k in range(chunks):
        at = pl.ds(k * group, group)
        loads.append(
            pltpu.make_async_copy(
                gathered.at[at, pl.ds(0, rows), :], masters.at[at], master_sem.at[k]
            )
        )
        loads[k].start()

    stores = []

    def store(source, target, sem):
        stores.append(pltpu.make_async_copy(source, target, sem))
        stores[-1].start()

    for item in inputs[:3]:
        item.wait()
    total = jnp.sum(squares[...], axis=0)[:1, :1]
    scale = 1.0 / jnp.sqrt(total / (R * (DK + DV)) + norm_eps)

    nf, ns = moments(low[...].astype(f32), scale, all_first[...].astype(f32), all_second[...].astype(f32))
    direction[...] = (nf / (jnp.sqrt(ns) + epsilon)).astype(bf16)

    for item in inputs[3:]:
        item.wait()
    nf_ks[...], ns_ks[...] = moments(own_low[:, :kc], scale, fk[...], sk[...])
    nf_vs[...], ns_vs[...] = moments(own_low[:, kc:], scale, fv[...], sv[...])
    step = dot(basis[...], direction[...])
    step_ks[...] = step[:, :kc]
    step_vs[...] = step[:, kc:]
    new_ks[...] = mk[...] - learn_rate * step[:, :kc]
    new_vs[...] = mv[...] - learn_rate * step[:, kc:]
    sources = (step_ks, step_vs, new_ks, new_vs, nf_ks, ns_ks, nf_vs, ns_vs)
    targets = (step_k, step_v, new_k, new_v, nf_k, ns_k, nf_v, ns_v)
    for k in range(len(sources)):
        store(sources[k], targets[k], own_sem.at[k])

    at = pl.multiple_of(core[0] * half, half)
    at_other = pl.multiple_of((1 - core[0]) * half, half)
    ordered = jnp.concatenate(
        [direction[pl.ds(at, half), :], direction[pl.ds(at_other, half), :]], axis=0
    )
    for k in range(chunks):
        size = group * rows
        at = pl.ds(k * size, size)
        both = jnp.concatenate([b_mine[at, :], b_other[at, :]], axis=1)
        step = dot(both, ordered)
        loads[k].wait()
        master = masters[pl.ds(k * group, group)].astype(f32).reshape(size, -1)
        copy = (master - learn_rate * step).astype(bf16)
        out_k[at, :] = copy[:, :kc]
        out_v[at, :] = copy[:, kc:]
        store(out_k.at[at], copy_k.at[at], out_sem.at[0, k])
        store(out_v.at[at], copy_v.at[at], out_sem.at[1, k])
    for item in stores:
        item.wait()


def to_everyone(array, axis):
    copies = jnp.broadcast_to(array, (lax.axis_size(axis), *array.shape))
    return lax.all_to_all(copies, axis, split_axis=0, concat_axis=0, tiled=True)


def on_device(normed, key_cot, value_cot, basis, mk, mv, fk, sk, fv, sv):
    kc = key_cot.shape[1]
    cols = kc + value_cot.shape[1]
    rows = basis.shape[0]
    d = normed.shape[1]
    own = fk.shape[0]
    n_fs = lax.axis_size(FS)
    n_tp = lax.axis_size(TP)
    half = R // 2
    core = lax.axis_index("tp_1").astype(jnp.int32).reshape(1)
    per = rows + 2 * own
    pair = [(0, 1), (1, 0)]

    pack, copies = pl.pallas_call(
        pack_kernel,
        out_shape=(shape((per, cols), bf16), shape((n_fs, rows, half), bf16)),
        in_specs=[SMEM] + [VMEM] * 7,
        out_specs=(VMEM, VMEM),
        compiler_params=limit(24),
        name="pack",
    )(core, *(in_hbm(x) for x in (mk, mv, fk, fv, sk, sv, basis)))
    block = pack
    for axis in PAIRS:
        other_block = lax.ppermute(block, axis, pair)
        block = pl.pallas_call(
            pair_kernel,
            out_shape=shape((2, *block.shape), bf16),
            in_specs=[SMEM] + [VMEM] * 2,
            out_specs=VMEM,
            compiler_params=limit(24),
            name="pair",
        )(lax.axis_index(axis).astype(jnp.int32).reshape(1), block, other_block)
        block = block.reshape(-1, cols)
    gathered = lax.all_gather(block, RING, axis=0, tiled=True).reshape(n_fs, per, cols)
    basis_mine = lax.all_to_all(copies, FS, 0, 0, tiled=True).reshape(d, half)

    cot = jnp.concatenate([key_cot, value_cot], axis=1)
    grad = lax.dot_general(cot, normed, (((0,), (0,)), ((), ())), preferred_element_type=f32)
    hi = grad.astype(bf16)
    lo = (grad - hi.astype(f32)).astype(bf16)
    basis_mine, hi, lo = lax.optimization_barrier((basis_mine, hi, lo))
    basis_other = lax.ppermute(basis_mine, "tp_1", pair)
    project_cost = cost(4 * d * half * cols, 4 * d * cols + 2 * d * half)
    low_mine = pl.pallas_call(
        project_kernel,
        out_shape=shape((half, cols), f32),
        in_specs=[VMEM] * 3,
        out_specs=VMEM,
        cost_estimate=project_cost,
        compiler_params=limit(12),
        name="project_mine",
    )(hi, lo, basis_mine)
    parts, basis_other = pl.pallas_call(
        project_both_kernel,
        out_shape=(shape((R, cols), f32), pltpu.HBM((d, half), bf16)),
        in_specs=[SMEM] + [VMEM] * 4,
        out_specs=(VMEM, HBM),
        scratch_shapes=[pltpu.SemaphoreType.DMA],
        cost_estimate=project_cost,
        compiler_params=limit(12),
        name="project_other",
    )(core, hi, lo, basis_other, low_mine)
    tiles = lax.all_to_all(parts.reshape(n_fs, own, cols), FS, 0, 0, tiled=True)
    own_low = jnp.sum(tiles, axis=0)

    all_low = to_everyone(own_low.astype(bf16), FS).reshape(R, cols)
    local = pl.pallas_call(
        squares_kernel,
        out_shape=shape((n_tp, 8, 128), f32),
        in_specs=[VMEM],
        out_specs=VMEM,
        compiler_params=limit(4),
        name="squares",
    )(all_low)
    squares = lax.all_to_all(local, TP, 0, 0, tiled=True)
    all_first, all_second = pl.pallas_call(
        prep_kernel,
        out_shape=(shape((R, cols), bf16), shape((R, cols), bf16)),
        in_specs=[ANY],
        out_specs=(VMEM, VMEM),
        scratch_shapes=[
            pltpu.VMEM((n_fs, 2 * own, cols), bf16),
            pltpu.SemaphoreType.DMA,
        ],
        cost_estimate=cost(4 * R * 2 * R * cols, 2 * n_fs * per * cols),
        compiler_params=limit(24),
        name="prep",
    )(in_hbm(gathered))

    chunks = 8
    vc = cols - kc
    small = ((rows, kc), (rows, vc)) * 2 + ((own, kc), (own, kc), (own, vc), (own, vc))
    outs = tuple(shape(dims, f32) for dims in small)
    return pl.pallas_call(
        final_kernel,
        out_shape=outs[:4] + (shape((d, kc), bf16), shape((d, vc), bf16)) + outs[4:],
        in_specs=[SMEM, VMEM] + [ANY] * 14,
        out_specs=(HBM,) * 10,
        scratch_shapes=[
            pltpu.VMEM((R, cols), bf16),
            pltpu.VMEM((R, cols), bf16),
            pltpu.VMEM((R, cols), bf16),
            pltpu.VMEM((own, cols), f32),
            pltpu.VMEM((own, kc), f32),
            pltpu.VMEM((own, vc), f32),
            pltpu.VMEM((own, kc), f32),
            pltpu.VMEM((own, vc), f32),
            pltpu.VMEM((rows, R), bf16),
            pltpu.VMEM((rows, kc), f32),
            pltpu.VMEM((rows, vc), f32),
            pltpu.VMEM((d, half), bf16),
            pltpu.VMEM((d, half), bf16),
            pltpu.VMEM((n_fs, rows, cols), bf16),
            pltpu.VMEM((R, cols), bf16),
            pltpu.VMEM((d, kc), bf16),
            pltpu.VMEM((d, vc), bf16),
        ]
        + [pltpu.VMEM(dims, f32) for dims in small]
        + [
            pltpu.SemaphoreType.DMA((13,)),
            pltpu.SemaphoreType.DMA((chunks,)),
            pltpu.SemaphoreType.DMA((2, chunks)),
            pltpu.SemaphoreType.DMA((8,)),
        ],
        compiler_params=limit(40),
        name="update",
    )(
        core, squares, all_low, all_first, all_second, own_low,
        *(in_hbm(x) for x in (fk, fv, sk, sv, basis, mk, mv, basis_mine, basis_other, gathered)),
    )


def solution(mesh):
    names = (*FS, *TP)
    torus = Mesh(mesh.devices.reshape(8, 2, 2, 2, 4, 2), names)
    split = P(FS, TP)
    in_specs = (P(FS, None), split, split, P(FS, None)) + (split,) * 6
    out_specs = (split,) * 4 + (P(None, TP),) * 2 + (split,) * 4
    return jax.shard_map(
        on_device, mesh=torus, in_specs=in_specs, out_specs=out_specs, check_vma=False
    )
```

```python
import jax
import jax.numpy as jnp
from jax import lax
from jax.experimental import pallas as pl
from jax.experimental.pallas import tpu as pltpu
from jax.sharding import Mesh
from jax.sharding import PartitionSpec as P

DK = 1024
DV = 2048
R = 256
FS = ("fs_0", "fs_1", "fs_2", "fs_3")
RING = ("fs_0", "fs_2")
NEAR = ("fs_1", "fs_3")
TP = ("tp_0", "tp_1")

learn_rate = 0.05
beta_first = 0.9
beta_second = 0.9
epsilon = 1e-08
norm_eps = 1e-06


f32 = jnp.float32
bf16 = jnp.bfloat16
VMEM = pl.BlockSpec(memory_space=pltpu.VMEM)
SMEM = pl.BlockSpec(memory_space=pltpu.SMEM)
ANY = pl.BlockSpec(memory_space=pl.ANY)
HBM = pl.BlockSpec(memory_space=pltpu.HBM)


def shape(dims, dtype):
    return jax.ShapeDtypeStruct(dims, dtype)


def cost(flops, moved):
    return pl.CostEstimate(flops=flops, bytes_accessed=moved, transcendentals=0)


def in_hbm(array):
    return pltpu.with_memory_space_constraint(array, pltpu.HBM)


def limit(mib):
    return pltpu.CompilerParams(vmem_limit_bytes=mib * 1024 * 1024)


def dot(a, b):
    return jnp.dot(a, b, preferred_element_type=f32)


def pack_kernel(core, mk, mv, fk, fv, sk, sv, basis, packs, copies):
    kc = mk.shape[1]
    rows, half = copies.shape[1], copies.shape[2]
    keys = jnp.concatenate([fk[...], sk[...]], axis=0).astype(bf16)
    values = jnp.concatenate([fv[...], sv[...]], axis=0).astype(bf16)
    for k in range(packs.shape[0]):
        packs[k, :rows, :kc] = mk[...].astype(bf16)
        packs[k, :rows, kc:] = mv[...].astype(bf16)
        packs[k, rows:, :kc] = keys
        packs[k, rows:, kc:] = values
    mine = jnp.where(core[0] == 0, basis[:, :half].astype(f32), basis[:, half:].astype(f32))
    copies[...] = jnp.broadcast_to(mine.astype(bf16)[None], copies.shape)


def project_kernel(hi, lo, basis, out):
    b = basis[...]
    out[...] = (dot(hi[...], b) + dot(lo[...], b)).T


def project_both_kernel(core, hi, lo, basis, mine, out, kept, sem):
    half = mine.shape[0]
    keep = pltpu.make_async_copy(basis, kept, sem)
    keep.start()
    b = basis[...]
    at = pl.multiple_of(core[0] * half, half)
    other = pl.multiple_of((1 - core[0]) * half, half)
    out[pl.ds(at, half), :] = mine[...].astype(bf16)
    out[pl.ds(other, half), :] = (dot(hi[...], b) + dot(lo[...], b)).T.astype(bf16)
    keep.wait()


def squares_kernel(low, out):
    x = low[...].astype(f32)
    out[...] = jnp.broadcast_to(jnp.sum(x * x, keepdims=True)[None], out.shape)


def moments(low, scale, first, second):
    scaled = low * scale
    new_first = beta_first * first + (1.0 - beta_first) * scaled
    new_second = beta_second * second + (1.0 - beta_second) * scaled * scaled
    return new_first, new_second


def row_loads(gathered, start, size, target, sems):
    zs, _, near, _, _, _ = gathered.shape
    for z in range(zs * near):
        source = gathered.at[z // near, :, z % near, :, pl.ds(start, size), :]
        yield pltpu.make_async_copy(source, target.at[z], sems.at[z])


def prep_kernel(gathered, first, second, mom, sems):
    per, cols = mom.shape[-2:]
    own = per // 2
    loads = list(row_loads(gathered, gathered.shape[4] - per, per, mom, sems))
    for load in loads:
        load.start()
    kept = first.shape[0]
    i = lax.broadcasted_iota(jnp.int32, (kept, 2 * kept), 0)
    j = lax.broadcasted_iota(jnp.int32, (kept, 2 * kept), 1)
    at_first = (i // own) * per + i % own
    pick_first = jnp.where(j == at_first, 1.0, 0.0).astype(bf16)
    pick_second = jnp.where(j == at_first + own, 1.0, 0.0).astype(bf16)
    for load in loads:
        load.wait()
    both = mom[...].reshape(2 * kept, cols)
    first[...] = dot(pick_first, both).astype(bf16)
    second[...] = dot(pick_second, both).astype(bf16)


def final_kernel(
    core, squares, low_h, all_first_h, all_second_h, own_low_h, fk_h, fv_h, sk_h, sv_h, basis_h, mk_h, mv_h,
    b_mine_h, b_other_h, gathered,
    step_k, step_v, new_k, new_v, copy_k, copy_v, nf_k, ns_k, nf_v, ns_v,
    low, all_first, all_second, own_low, fk, fv, sk, sv, basis, mk, mv, b_mine, b_other,
    masters, direction, out_k, out_v,
    step_ks, step_vs, new_ks, new_vs, nf_ks, ns_ks, nf_vs, ns_vs, in_sem, master_sem, out_sem, own_sem,
):
    rows = mk.shape[0]
    kc = mk.shape[1]
    half = b_mine.shape[1]
    chunks = masters.shape[0]
    size = copy_k.shape[0] // chunks
    here = (low, all_first, all_second, own_low, fk, fv, sk, sv, basis, mk, mv, b_mine, b_other)
    there = (
        low_h, all_first_h, all_second_h, own_low_h, fk_h, fv_h, sk_h, sv_h, basis_h, mk_h, mv_h,
        b_mine_h, b_other_h,
    )
    inputs = []
    for k in range(len(here)):
        inputs.append(pltpu.make_async_copy(there[k], here[k], in_sem.at[k]))
        inputs[k].start()
    loads = list(row_loads(gathered, 0, rows, masters, master_sem))
    for load in loads:
        load.start()

    stores = []

    def store(source, target, sem):
        stores.append(pltpu.make_async_copy(source, target, sem))
        stores[-1].start()

    for item in inputs[:3]:
        item.wait()
    total = jnp.sum(squares[...], axis=0)[:1, :1]
    scale = 1.0 / jnp.sqrt(total / (R * (DK + DV)) + norm_eps)

    nf, ns = moments(low[...].astype(f32), scale, all_first[...].astype(f32), all_second[...].astype(f32))
    direction[...] = (nf / (jnp.sqrt(ns) + epsilon)).astype(bf16)

    for item in inputs[3:]:
        item.wait()
    nf_ks[...], ns_ks[...] = moments(own_low[:, :kc], scale, fk[...], sk[...])
    nf_vs[...], ns_vs[...] = moments(own_low[:, kc:], scale, fv[...], sv[...])
    step = dot(basis[...], direction[...])
    step_ks[...] = step[:, :kc]
    step_vs[...] = step[:, kc:]
    new_ks[...] = mk[...] - learn_rate * step[:, :kc]
    new_vs[...] = mv[...] - learn_rate * step[:, kc:]
    sources = (step_ks, step_vs, new_ks, new_vs, nf_ks, ns_ks, nf_vs, ns_vs)
    targets = (step_k, step_v, new_k, new_v, nf_k, ns_k, nf_v, ns_v)
    for k in range(len(sources)):
        store(sources[k], targets[k], own_sem.at[k])

    at = pl.multiple_of(core[0] * half, half)
    at_other = pl.multiple_of((1 - core[0]) * half, half)
    ordered = jnp.concatenate(
        [direction[pl.ds(at, half), :], direction[pl.ds(at_other, half), :]], axis=0
    )
    for k in range(chunks):
        at = pl.ds(k * size, size)
        both = jnp.concatenate([b_mine[at, :], b_other[at, :]], axis=1)
        step = dot(both, ordered)
        loads[k].wait()
        master = masters[k].astype(f32).reshape(size, -1)
        copy = (master - learn_rate * step).astype(bf16)
        out_k[at, :] = copy[:, :kc]
        out_v[at, :] = copy[:, kc:]
        store(out_k.at[at], copy_k.at[at], out_sem.at[0, k])
        store(out_v.at[at], copy_v.at[at], out_sem.at[1, k])
    for item in stores:
        item.wait()


def to_everyone(array, axis):
    copies = jnp.broadcast_to(array, (lax.axis_size(axis), *array.shape))
    return lax.all_to_all(copies, axis, split_axis=0, concat_axis=0, tiled=True)


def on_device(normed, key_cot, value_cot, basis, mk, mv, fk, sk, fv, sv):
    kc = key_cot.shape[1]
    cols = kc + value_cot.shape[1]
    rows = basis.shape[0]
    d = normed.shape[1]
    own = fk.shape[0]
    n_fs = lax.axis_size(FS)
    n_tp = lax.axis_size(TP)
    half = R // 2
    core = lax.axis_index("tp_1").astype(jnp.int32).reshape(1)
    per = rows + 2 * own
    pair = [(0, 1), (1, 0)]

    near = lax.axis_size(NEAR)
    packs, copies = pl.pallas_call(
        pack_kernel,
        out_shape=(shape((near, per, cols), bf16), shape((n_fs, rows, half), bf16)),
        in_specs=[SMEM] + [VMEM] * 7,
        out_specs=(VMEM, VMEM),
        compiler_params=limit(24),
        name="pack",
    )(core, *(in_hbm(x) for x in (mk, mv, fk, fv, sk, sv, basis)))
    block = lax.all_to_all(packs, NEAR, 0, 0, tiled=True).reshape(near * per, cols)
    gathered = lax.all_gather(block, RING, axis=0, tiled=True)
    zs, ys = lax.axis_size("fs_0"), lax.axis_size("fs_2")
    z_near, y_near = lax.axis_size("fs_1"), lax.axis_size("fs_3")
    gathered = gathered.reshape(zs, ys, z_near, y_near, per, cols)
    chunks = zs * z_near
    basis_mine = lax.all_to_all(copies, FS, 0, 0, tiled=True).reshape(d, half)

    cot = jnp.concatenate([key_cot, value_cot], axis=1)
    grad = lax.dot_general(cot, normed, (((0,), (0,)), ((), ())), preferred_element_type=f32)
    hi = grad.astype(bf16)
    lo = (grad - hi.astype(f32)).astype(bf16)
    basis_mine, hi, lo = lax.optimization_barrier((basis_mine, hi, lo))
    basis_other = lax.ppermute(basis_mine, "tp_1", pair)
    project_cost = cost(4 * d * half * cols, 4 * d * cols + 2 * d * half)
    low_mine = pl.pallas_call(
        project_kernel,
        out_shape=shape((half, cols), f32),
        in_specs=[VMEM] * 3,
        out_specs=VMEM,
        cost_estimate=project_cost,
        compiler_params=limit(12),
        name="project_mine",
    )(hi, lo, basis_mine)
    parts, basis_other = pl.pallas_call(
        project_both_kernel,
        out_shape=(shape((R, cols), bf16), pltpu.HBM((d, half), bf16)),
        in_specs=[SMEM] + [VMEM] * 4,
        out_specs=(VMEM, HBM),
        scratch_shapes=[pltpu.SemaphoreType.DMA],
        cost_estimate=project_cost,
        compiler_params=limit(12),
        name="project_other",
    )(core, hi, lo, basis_other, low_mine)
    tiles = lax.all_to_all(parts.reshape(n_fs, own, cols), FS, 0, 0, tiled=True)
    own_low = jnp.sum(tiles.astype(f32), axis=0)

    all_low = to_everyone(own_low.astype(bf16), FS).reshape(R, cols)
    local = pl.pallas_call(
        squares_kernel,
        out_shape=shape((n_tp, 8, 128), f32),
        in_specs=[VMEM],
        out_specs=VMEM,
        compiler_params=limit(4),
        name="squares",
    )(all_low)
    squares = lax.all_to_all(local, TP, 0, 0, tiled=True)
    all_first, all_second = pl.pallas_call(
        prep_kernel,
        out_shape=(shape((R, cols), bf16), shape((R, cols), bf16)),
        in_specs=[ANY],
        out_specs=(VMEM, VMEM),
        scratch_shapes=[
            pltpu.VMEM((chunks, ys, y_near, 2 * own, cols), bf16),
            pltpu.SemaphoreType.DMA((chunks,)),
        ],
        cost_estimate=cost(4 * R * 2 * R * cols, 2 * n_fs * per * cols),
        compiler_params=limit(24),
        name="prep",
    )(in_hbm(gathered))

    vc = cols - kc
    small = ((rows, kc), (rows, vc)) * 2 + ((own, kc), (own, kc), (own, vc), (own, vc))
    outs = tuple(shape(dims, f32) for dims in small)
    return pl.pallas_call(
        final_kernel,
        out_shape=outs[:4] + (shape((d, kc), bf16), shape((d, vc), bf16)) + outs[4:],
        in_specs=[SMEM, VMEM] + [ANY] * 14,
        out_specs=(HBM,) * 10,
        scratch_shapes=[
            pltpu.VMEM((R, cols), bf16),
            pltpu.VMEM((R, cols), bf16),
            pltpu.VMEM((R, cols), bf16),
            pltpu.VMEM((own, cols), f32),
            pltpu.VMEM((own, kc), f32),
            pltpu.VMEM((own, vc), f32),
            pltpu.VMEM((own, kc), f32),
            pltpu.VMEM((own, vc), f32),
            pltpu.VMEM((rows, R), bf16),
            pltpu.VMEM((rows, kc), f32),
            pltpu.VMEM((rows, vc), f32),
            pltpu.VMEM((d, half), bf16),
            pltpu.VMEM((d, half), bf16),
            pltpu.VMEM((chunks, ys, y_near, rows, cols), bf16),
            pltpu.VMEM((R, cols), bf16),
            pltpu.VMEM((d, kc), bf16),
            pltpu.VMEM((d, vc), bf16),
        ]
        + [pltpu.VMEM(dims, f32) for dims in small]
        + [
            pltpu.SemaphoreType.DMA((13,)),
            pltpu.SemaphoreType.DMA((chunks,)),
            pltpu.SemaphoreType.DMA((2, chunks)),
            pltpu.SemaphoreType.DMA((8,)),
        ],
        compiler_params=limit(40),
        name="update",
    )(
        core, squares, all_low, all_first, all_second, own_low,
        *(in_hbm(x) for x in (fk, fv, sk, sv, basis, mk, mv, basis_mine, basis_other, gathered)),
    )


def solution(mesh):
    names = (*FS, *TP)
    torus = Mesh(mesh.devices.reshape(4, 2, 4, 2, 4, 2), names)
    split = P(FS, TP)
    in_specs = (P(FS, None), split, split, P(FS, None)) + (split,) * 6
    out_specs = (split,) * 4 + (P(None, TP),) * 2 + (split,) * 4
    return jax.shard_map(
        on_device, mesh=torus, in_specs=in_specs, out_specs=out_specs, check_vma=False
    )
```

```python
import jax
import jax.numpy as jnp
from jax import lax
from jax.experimental import pallas as pl
from jax.experimental.pallas import tpu as pltpu
from jax.sharding import Mesh
from jax.sharding import PartitionSpec as P

DK = 1024
DV = 2048
R = 256
FS = ("fs_0", "fs_1")
TP = ("tp_0", "tp_1")

learn_rate = 0.05
beta_first = 0.9
beta_second = 0.9
epsilon = 1e-08
norm_eps = 1e-06


f32 = jnp.float32
bf16 = jnp.bfloat16
VMEM = pl.BlockSpec(memory_space=pltpu.VMEM)
SMEM = pl.BlockSpec(memory_space=pltpu.SMEM)
ANY = pl.BlockSpec(memory_space=pl.ANY)
HBM = pl.BlockSpec(memory_space=pltpu.HBM)


def shape(dims, dtype):
    return jax.ShapeDtypeStruct(dims, dtype)


def cost(flops, moved):
    return pl.CostEstimate(flops=flops, bytes_accessed=moved, transcendentals=0)


def in_hbm(array):
    return pltpu.with_memory_space_constraint(array, pltpu.HBM)


def limit(mib):
    return pltpu.CompilerParams(vmem_limit_bytes=mib * 1024 * 1024)


def dot(a, b):
    return jnp.dot(a, b, preferred_element_type=f32)


def pack_kernel(mk, mv, fk, fv, sk, sv, pack):
    rows, kc = mk.shape
    pack[:rows, :kc] = mk[...].astype(bf16)
    pack[:rows, kc:] = mv[...].astype(bf16)
    pack[rows:, :kc] = jnp.concatenate([fk[...], sk[...]], axis=0).astype(bf16)
    pack[rows:, kc:] = jnp.concatenate([fv[...], sv[...]], axis=0).astype(bf16)


def copies_kernel(core, basis, copies):
    half = copies.shape[2]
    mine = jnp.where(core[0] == 0, basis[:, :half].astype(f32), basis[:, half:].astype(f32))
    copies[...] = jnp.broadcast_to(mine.astype(bf16)[None], copies.shape)


def project_kernel(hi, lo, basis, out):
    b = basis[...]
    out[...] = (dot(hi[...], b) + dot(lo[...], b)).T


def project_both_kernel(core, hi, lo, basis, mine, out, kept, sem):
    half = mine.shape[0]
    keep = pltpu.make_async_copy(basis, kept, sem)
    keep.start()
    b = basis[...]
    at = pl.multiple_of(core[0] * half, half)
    other = pl.multiple_of((1 - core[0]) * half, half)
    out[pl.ds(at, half), :] = mine[...]
    out[pl.ds(other, half), :] = (dot(hi[...], b) + dot(lo[...], b)).T
    keep.wait()


def squares_kernel(low, out):
    x = low[...].astype(f32)
    out[...] = jnp.broadcast_to(jnp.sum(x * x, keepdims=True)[None], out.shape)


def moments(low, scale, first, second):
    scaled = low * scale
    new_first = beta_first * first + (1.0 - beta_first) * scaled
    new_second = beta_second * second + (1.0 - beta_second) * scaled * scaled
    return new_first, new_second


def prep_kernel(
    core, mine, other, basis, mk, mv, fk, fv, sk, sv,
    full_basis, own_basis, master, first, second,
    mk_v, mv_v, fk_v, fv_v, sk_v, sv_v, sems,
):
    kc = mk.shape[1]
    half = mine.shape[1]
    at = pl.multiple_of(core[0] * half, half)
    at_other = pl.multiple_of((1 - core[0]) * half, half)
    loads = [
        pltpu.make_async_copy(mine, full_basis.at[:, pl.ds(at, half)], sems.at[0]),
        pltpu.make_async_copy(other, full_basis.at[:, pl.ds(at_other, half)], sems.at[1]),
        pltpu.make_async_copy(basis, own_basis, sems.at[2]),
        pltpu.make_async_copy(mk, mk_v, sems.at[3]),
        pltpu.make_async_copy(mv, mv_v, sems.at[4]),
        pltpu.make_async_copy(fk, fk_v, sems.at[5]),
        pltpu.make_async_copy(fv, fv_v, sems.at[6]),
        pltpu.make_async_copy(sk, sk_v, sems.at[7]),
        pltpu.make_async_copy(sv, sv_v, sems.at[8]),
    ]
    for load in loads:
        load.start()
    for load in loads:
        load.wait()
    master[:, :kc] = mk_v[...]
    master[:, kc:] = mv_v[...]
    first[:, :kc] = fk_v[...]
    first[:, kc:] = fv_v[...]
    second[:, :kc] = sk_v[...]
    second[:, kc:] = sv_v[...]


def final_kernel(
    squares, low, own_low, full_basis, basis, master, first, second, gathered,
    step_k, step_v, new_k, new_v, copy_k, copy_v, nf_k, ns_k, nf_v, ns_v,
    mom, masters, out_k, out_v,
    step_ks, step_vs, new_ks, new_vs, nf_ks, ns_ks, nf_vs, ns_vs, mom_sem, master_sem, out_sem, own_sem,
):
    n_fs, per, cols = mom.shape
    rows = master.shape[0]
    kc = step_k.shape[1]
    chunks = master_sem.shape[0]
    group = n_fs // chunks
    size = group * rows
    load = pltpu.make_async_copy(gathered.at[:, pl.ds(rows, per), :], mom, mom_sem)
    load.start()
    loads = []
    for k in range(chunks):
        at = pl.ds(k * group, group)
        source = gathered.at[at, pl.ds(0, rows), :]
        loads.append(pltpu.make_async_copy(source, masters.at[at], master_sem.at[k]))
        loads[k].start()

    stores = []

    def store(source, target, sem):
        stores.append(pltpu.make_async_copy(source, target, sem))
        stores[-1].start()

    total = jnp.sum(squares[...], axis=0)[:1, :1]
    scale = 1.0 / jnp.sqrt(total / (R * (DK + DV)) + norm_eps)
    nf, ns = moments(own_low[...], scale, first[...], second[...])
    nf_ks[...] = nf[:, :kc]
    nf_vs[...] = nf[:, kc:]
    ns_ks[...] = ns[:, :kc]
    ns_vs[...] = ns[:, kc:]

    own = per // 2
    i = lax.broadcasted_iota(jnp.int32, (n_fs * own, n_fs * per), 0)
    j = lax.broadcasted_iota(jnp.int32, (n_fs * own, n_fs * per), 1)
    at_first = (i // own) * per + i % own
    pick_first = jnp.where(j == at_first, 1.0, 0.0).astype(bf16)
    pick_second = jnp.where(j == at_first + own, 1.0, 0.0).astype(bf16)
    load.wait()
    both = mom[...].reshape(n_fs * per, cols)
    nf, ns = moments(low[...].astype(f32), scale, dot(pick_first, both), dot(pick_second, both))
    direction = (nf / (jnp.sqrt(ns) + epsilon)).astype(bf16)

    for k in range(chunks):
        at = pl.ds(k * size, size)
        step = dot(full_basis[at, :], direction)
        loads[k].wait()
        old = masters[pl.ds(k * group, group)].astype(f32).reshape(size, cols)
        copy = (old - learn_rate * step).astype(bf16)
        out_k[at, :] = copy[:, :kc]
        out_v[at, :] = copy[:, kc:]
        store(out_k.at[at], copy_k.at[at], out_sem.at[0, k])
        store(out_v.at[at], copy_v.at[at], out_sem.at[1, k])
        if k == 0:
            step = dot(basis[...], direction)
            step_ks[...] = step[:, :kc]
            step_vs[...] = step[:, kc:]
            new = master[...] - learn_rate * step
            new_ks[...] = new[:, :kc]
            new_vs[...] = new[:, kc:]
            sources = (step_ks, step_vs, new_ks, new_vs, nf_ks, ns_ks, nf_vs, ns_vs)
            targets = (step_k, step_v, new_k, new_v, nf_k, ns_k, nf_v, ns_v)
            for n in range(len(sources)):
                store(sources[n], targets[n], own_sem.at[n])
    for item in stores:
        item.wait()


def to_everyone(array, axis):
    copies = jnp.broadcast_to(array, (lax.axis_size(axis), *array.shape))
    return lax.all_to_all(copies, axis, split_axis=0, concat_axis=0, tiled=True)


def on_device(normed, key_cot, value_cot, basis, mk, mv, fk, sk, fv, sv):
    kc = key_cot.shape[1]
    cols = kc + value_cot.shape[1]
    rows = basis.shape[0]
    d = normed.shape[1]
    own = fk.shape[0]
    n_fs = lax.axis_size(FS)
    n_tp = lax.axis_size(TP)
    half = R // 2
    core = lax.axis_index("tp_1").astype(jnp.int32).reshape(1)
    per = rows + 2 * own
    pair = [(0, 1), (1, 0)]

    pack = pl.pallas_call(
        pack_kernel,
        out_shape=shape((per, cols), bf16),
        in_specs=[VMEM] * 6,
        out_specs=VMEM,
        compiler_params=limit(24),
        name="pack",
    )(*(in_hbm(x) for x in (mk, mv, fk, fv, sk, sv)))
    gathered = lax.all_gather(pack, FS, axis=0, tiled=True).reshape(n_fs, per, cols)
    copies = pl.pallas_call(
        copies_kernel,
        out_shape=shape((n_fs, rows, half), bf16),
        in_specs=[SMEM, VMEM],
        out_specs=VMEM,
        compiler_params=limit(24),
        name="copies",
    )(core, in_hbm(basis))
    basis_mine = lax.all_to_all(copies, FS, 0, 0, tiled=True).reshape(d, half)

    cot = jnp.concatenate([key_cot, value_cot], axis=1)
    grad = lax.dot_general(cot, normed, (((0,), (0,)), ((), ())), preferred_element_type=f32)
    hi = grad.astype(bf16)
    lo = (grad - hi.astype(f32)).astype(bf16)
    basis_mine, hi, lo = lax.optimization_barrier((basis_mine, hi, lo))
    basis_other = lax.ppermute(basis_mine, "tp_1", pair)
    project_cost = cost(4 * d * half * cols, 4 * d * cols + 2 * d * half)
    low_mine = pl.pallas_call(
        project_kernel,
        out_shape=shape((half, cols), f32),
        in_specs=[VMEM] * 3,
        out_specs=VMEM,
        cost_estimate=project_cost,
        compiler_params=limit(12),
        name="project_mine",
    )(hi, lo, basis_mine)
    parts, basis_other = pl.pallas_call(
        project_both_kernel,
        out_shape=(shape((R, cols), f32), pltpu.HBM((d, half), bf16)),
        in_specs=[SMEM] + [VMEM] * 4,
        out_specs=(VMEM, HBM),
        scratch_shapes=[pltpu.SemaphoreType.DMA],
        cost_estimate=project_cost,
        compiler_params=limit(12),
        name="project_other",
    )(core, hi, lo, basis_other, low_mine)
    tiles = lax.all_to_all(parts.reshape(n_fs, own, cols), FS, 0, 0, tiled=True)
    own_low = jnp.sum(tiles.astype(f32), axis=0)

    all_low = to_everyone(own_low.astype(bf16), FS).reshape(R, cols)
    local = pl.pallas_call(
        squares_kernel,
        out_shape=shape((n_tp, 8, 128), f32),
        in_specs=[VMEM],
        out_specs=VMEM,
        compiler_params=limit(4),
        name="squares",
    )(all_low)
    squares = lax.all_to_all(local, TP, 0, 0, tiled=True)
    vc = cols - kc
    small = ((rows, kc), (rows, vc)) * 2 + ((own, kc), (own, kc), (own, vc), (own, vc))
    held = pl.pallas_call(
        prep_kernel,
        out_shape=(
            shape((d, R), bf16),
            shape((rows, R), bf16),
            shape((rows, cols), f32),
            shape((own, cols), f32),
            shape((own, cols), f32),
        ),
        in_specs=[SMEM] + [ANY] * 9,
        out_specs=(VMEM,) * 5,
        scratch_shapes=[
            pltpu.VMEM((rows, kc), f32),
            pltpu.VMEM((rows, vc), f32),
            pltpu.VMEM((own, kc), f32),
            pltpu.VMEM((own, vc), f32),
            pltpu.VMEM((own, kc), f32),
            pltpu.VMEM((own, vc), f32),
            pltpu.SemaphoreType.DMA((9,)),
        ],
        cost_estimate=cost(4 * R * 2 * R * cols, 4 * d * R),
        compiler_params=limit(24),
        name="prep",
    )(core, *(in_hbm(x) for x in (basis_mine, basis_other, basis, mk, mv, fk, fv, sk, sv)))

    chunks = 8
    outs = tuple(shape(dims, f32) for dims in small)
    return pl.pallas_call(
        final_kernel,
        out_shape=outs[:4] + (shape((d, kc), bf16), shape((d, vc), bf16)) + outs[4:],
        in_specs=[VMEM] * 8 + [ANY],
        out_specs=(HBM,) * 10,
        scratch_shapes=[
            pltpu.VMEM((n_fs, 2 * own, cols), bf16),
            pltpu.VMEM((n_fs, rows, cols), bf16),
            pltpu.VMEM((d, kc), bf16),
            pltpu.VMEM((d, vc), bf16),
        ]
        + [pltpu.VMEM(dims, f32) for dims in small]
        + [
            pltpu.SemaphoreType.DMA,
            pltpu.SemaphoreType.DMA((chunks,)),
            pltpu.SemaphoreType.DMA((2, chunks)),
            pltpu.SemaphoreType.DMA((8,)),
        ],
        compiler_params=limit(32),
        name="update",
    )(squares, all_low, own_low, *held, in_hbm(gathered))


def solution(mesh):
    names = (*FS, *TP)
    torus = Mesh(mesh.devices.reshape(8, 8, 4, 2), names)
    split = P(FS, TP)
    in_specs = (P(FS, None), split, split, P(FS, None)) + (split,) * 6
    out_specs = (split,) * 4 + (P(None, TP),) * 2 + (split,) * 4
    return jax.shard_map(
        on_device, mesh=torus, in_specs=in_specs, out_specs=out_specs, check_vma=False
    )
```

```python
import jax
import jax.numpy as jnp
from jax import lax
from jax.experimental import pallas as pl
from jax.experimental.pallas import tpu as pltpu
from jax.sharding import Mesh
from jax.sharding import PartitionSpec as P

DK = 1024
DV = 2048
R = 256
FS = ("fs_0", "fs_1")
TP = ("tp_0", "tp_1")

learn_rate = 0.05
beta_first = 0.9
beta_second = 0.9
epsilon = 1e-08
norm_eps = 1e-06


f32 = jnp.float32
bf16 = jnp.bfloat16
VMEM = pl.BlockSpec(memory_space=pltpu.VMEM)
SMEM = pl.BlockSpec(memory_space=pltpu.SMEM)
ANY = pl.BlockSpec(memory_space=pl.ANY)
HBM = pl.BlockSpec(memory_space=pltpu.HBM)


def shape(dims, dtype):
    return jax.ShapeDtypeStruct(dims, dtype)


def cost(flops, moved):
    return pl.CostEstimate(flops=flops, bytes_accessed=moved, transcendentals=0)


def in_hbm(array):
    return pltpu.with_memory_space_constraint(array, pltpu.HBM)


def limit(mib):
    return pltpu.CompilerParams(vmem_limit_bytes=mib * 1024 * 1024)


def dot(a, b):
    return jnp.dot(a, b, preferred_element_type=f32)


def pack_kernel(core, mk, mv, fk, fv, sk, sv, basis, pack, copies):
    rows, kc = mk.shape
    half = copies.shape[2]
    mine = jnp.where(core[0] == 0, basis[:, :half].astype(f32), basis[:, half:].astype(f32))
    copies[...] = jnp.broadcast_to(mine.astype(bf16)[None], copies.shape)
    pack[:rows, :kc] = mk[...].astype(bf16)
    pack[:rows, kc:] = mv[...].astype(bf16)
    pack[rows:, :kc] = jnp.concatenate([fk[...], sk[...]], axis=0).astype(bf16)
    pack[rows:, kc:] = jnp.concatenate([fv[...], sv[...]], axis=0).astype(bf16)


def project_kernel(hi, lo, basis, out, held, sems):
    chunks = sems.shape[0]
    depth = held.shape[0] // chunks
    spans = [pl.ds(k * depth, depth) for k in range(chunks)]
    loads = [pltpu.make_async_copy(basis.at[at], held.at[at], sems.at[k]) for k, at in enumerate(spans)]
    for load in loads:
        load.start()
    total = jnp.zeros((hi.shape[0], held.shape[1]), f32)
    for load, at in zip(loads, spans):
        load.wait()
        total += dot(hi[:, at], held[at, :]) + dot(lo[:, at], held[at, :])
    out[...] = total.T


def project_both_kernel(core, hi, lo, basis, mine, out, kept, sem):
    half = mine.shape[0]
    keep = pltpu.make_async_copy(basis, kept, sem)
    keep.start()
    b = basis[...]
    at = pl.multiple_of(core[0] * half, half)
    other = pl.multiple_of((1 - core[0]) * half, half)
    out[pl.ds(at, half), :] = mine[...]
    out[pl.ds(other, half), :] = (dot(hi[...], b) + dot(lo[...], b)).T
    keep.wait()


def squares_kernel(low, out):
    x = low[...].astype(f32)
    out[...] = jnp.broadcast_to(jnp.sum(x * x, keepdims=True)[None], out.shape)


def moments(low, scale, first, second):
    scaled = low * scale
    new_first = beta_first * first + (1.0 - beta_first) * scaled
    new_second = beta_second * second + (1.0 - beta_second) * scaled * scaled
    return new_first, new_second


def prep_kernel(
    core, mine, other, basis, mk, mv, fk, fv, sk, sv,
    full_basis, own_basis, master, first, second,
    mk_v, mv_v, fk_v, fv_v, sk_v, sv_v, sems,
):
    kc = mk.shape[1]
    half = mine.shape[1]
    at = pl.multiple_of(core[0] * half, half)
    at_other = pl.multiple_of((1 - core[0]) * half, half)
    loads = [
        pltpu.make_async_copy(mine, full_basis.at[:, pl.ds(at, half)], sems.at[0]),
        pltpu.make_async_copy(other, full_basis.at[:, pl.ds(at_other, half)], sems.at[1]),
        pltpu.make_async_copy(basis, own_basis, sems.at[2]),
        pltpu.make_async_copy(mk, mk_v, sems.at[3]),
        pltpu.make_async_copy(mv, mv_v, sems.at[4]),
        pltpu.make_async_copy(fk, fk_v, sems.at[5]),
        pltpu.make_async_copy(fv, fv_v, sems.at[6]),
        pltpu.make_async_copy(sk, sk_v, sems.at[7]),
        pltpu.make_async_copy(sv, sv_v, sems.at[8]),
    ]
    for load in loads:
        load.start()
    for load in loads:
        load.wait()
    master[:, :kc] = mk_v[...]
    master[:, kc:] = mv_v[...]
    first[:, :kc] = fk_v[...]
    first[:, kc:] = fv_v[...]
    second[:, :kc] = sk_v[...]
    second[:, kc:] = sv_v[...]


def final_kernel(
    squares, low, own_low, full_basis, basis, master, first, second, gathered,
    step_k, step_v, new_k, new_v, copy_k, copy_v, nf_k, ns_k, nf_v, ns_v,
    mom, masters, out_k, out_v,
    step_ks, step_vs, new_ks, new_vs, nf_ks, ns_ks, nf_vs, ns_vs, mom_sem, master_sem, out_sem, own_sem,
):
    n_fs, per, cols = mom.shape
    rows = master.shape[0]
    kc = step_k.shape[1]
    chunks = master_sem.shape[0]
    group = n_fs // chunks
    size = group * rows
    load = pltpu.make_async_copy(gathered.at[:, pl.ds(rows, per), :], mom, mom_sem)
    load.start()
    loads = []
    for k in range(chunks):
        at = pl.ds(k * group, group)
        source = gathered.at[at, pl.ds(0, rows), :]
        loads.append(pltpu.make_async_copy(source, masters.at[at], master_sem.at[k]))
        loads[k].start()

    stores = []

    def store(source, target, sem):
        stores.append(pltpu.make_async_copy(source, target, sem))
        stores[-1].start()

    total = jnp.sum(squares[...], axis=0)[:1, :1]
    scale = 1.0 / jnp.sqrt(total / (R * (DK + DV)) + norm_eps)
    nf, ns = moments(own_low[...], scale, first[...], second[...])
    nf_ks[...] = nf[:, :kc]
    nf_vs[...] = nf[:, kc:]
    ns_ks[...] = ns[:, :kc]
    ns_vs[...] = ns[:, kc:]

    own = per // 2
    i = lax.broadcasted_iota(jnp.int32, (n_fs * own, n_fs * per), 0)
    j = lax.broadcasted_iota(jnp.int32, (n_fs * own, n_fs * per), 1)
    at_first = (i // own) * per + i % own
    pick_first = jnp.where(j == at_first, 1.0, 0.0).astype(bf16)
    pick_second = jnp.where(j == at_first + own, 1.0, 0.0).astype(bf16)
    load.wait()
    both = mom[...].reshape(n_fs * per, cols)
    nf, ns = moments(low[...].astype(f32), scale, dot(pick_first, both), dot(pick_second, both))
    direction = (nf / (jnp.sqrt(ns) + epsilon)).astype(bf16)

    for k in range(chunks):
        at = pl.ds(k * size, size)
        step = dot(full_basis[at, :], direction)
        loads[k].wait()
        old = masters[pl.ds(k * group, group)].astype(f32).reshape(size, cols)
        copy = (old - learn_rate * step).astype(bf16)
        out_k[at, :] = copy[:, :kc]
        out_v[at, :] = copy[:, kc:]
        store(out_k.at[at], copy_k.at[at], out_sem.at[0, k])
        store(out_v.at[at], copy_v.at[at], out_sem.at[1, k])
        if k == 0:
            step = dot(basis[...], direction)
            step_ks[...] = step[:, :kc]
            step_vs[...] = step[:, kc:]
            new = master[...] - learn_rate * step
            new_ks[...] = new[:, :kc]
            new_vs[...] = new[:, kc:]
            sources = (step_ks, step_vs, new_ks, new_vs, nf_ks, ns_ks, nf_vs, ns_vs)
            targets = (step_k, step_v, new_k, new_v, nf_k, ns_k, nf_v, ns_v)
            for n in range(len(sources)):
                store(sources[n], targets[n], own_sem.at[n])
    for item in stores:
        item.wait()


def to_everyone(array, axis):
    copies = jnp.broadcast_to(array, (lax.axis_size(axis), *array.shape))
    return lax.all_to_all(copies, axis, split_axis=0, concat_axis=0, tiled=True)


def on_device(normed, key_cot, value_cot, basis, mk, mv, fk, sk, fv, sv):
    kc = key_cot.shape[1]
    cols = kc + value_cot.shape[1]
    rows = basis.shape[0]
    d = normed.shape[1]
    own = fk.shape[0]
    n_fs = lax.axis_size(FS)
    n_tp = lax.axis_size(TP)
    half = R // 2
    core = lax.axis_index("tp_1").astype(jnp.int32).reshape(1)
    per = rows + 2 * own
    pair = [(0, 1), (1, 0)]

    pack, copies = pl.pallas_call(
        pack_kernel,
        out_shape=(shape((per, cols), bf16), shape((n_fs, rows, half), bf16)),
        in_specs=[SMEM] + [VMEM] * 7,
        out_specs=(VMEM, VMEM),
        compiler_params=limit(24),
        name="pack",
    )(core, *(in_hbm(x) for x in (mk, mv, fk, fv, sk, sv, basis)))
    gathered = lax.all_gather(pack, FS, axis=0, tiled=True).reshape(n_fs, per, cols)
    basis_mine = lax.all_to_all(copies, FS, 0, 0, tiled=True).reshape(d, half)

    cot = jnp.concatenate([key_cot, value_cot], axis=1)
    grad = lax.dot_general(cot, normed, (((0,), (0,)), ((), ())), preferred_element_type=f32)
    hi = grad.astype(bf16)
    lo = (grad - hi.astype(f32)).astype(bf16)
    basis_mine, hi, lo = lax.optimization_barrier((basis_mine, hi, lo))
    basis_other = lax.ppermute(basis_mine, "tp_1", pair)
    project_cost = cost(4 * d * half * cols, 4 * d * cols + 2 * d * half)
    low_mine = pl.pallas_call(
        project_kernel,
        out_shape=shape((half, cols), f32),
        in_specs=[VMEM] * 2 + [ANY],
        out_specs=VMEM,
        scratch_shapes=[pltpu.VMEM((d, half), bf16), pltpu.SemaphoreType.DMA((4,))],
        cost_estimate=project_cost,
        compiler_params=limit(12),
        name="project_mine",
    )(hi, lo, in_hbm(basis_mine))
    parts, basis_other = pl.pallas_call(
        project_both_kernel,
        out_shape=(shape((R, cols), f32), pltpu.HBM((d, half), bf16)),
        in_specs=[SMEM] + [VMEM] * 4,
        out_specs=(VMEM, HBM),
        scratch_shapes=[pltpu.SemaphoreType.DMA],
        cost_estimate=project_cost,
        compiler_params=limit(12),
        name="project_other",
    )(core, hi, lo, basis_other, low_mine)
    tiles = lax.all_to_all(parts.reshape(n_fs, own, cols), FS, 0, 0, tiled=True)
    own_low = jnp.sum(tiles.astype(f32), axis=0)

    all_low = to_everyone(own_low.astype(bf16), FS).reshape(R, cols)
    local = pl.pallas_call(
        squares_kernel,
        out_shape=shape((n_tp, 8, 128), f32),
        in_specs=[VMEM],
        out_specs=VMEM,
        compiler_params=limit(4),
        name="squares",
    )(all_low)
    squares = lax.all_to_all(local, TP, 0, 0, tiled=True)
    vc = cols - kc
    small = ((rows, kc), (rows, vc)) * 2 + ((own, kc), (own, kc), (own, vc), (own, vc))
    held = pl.pallas_call(
        prep_kernel,
        out_shape=(
            shape((d, R), bf16),
            shape((rows, R), bf16),
            shape((rows, cols), f32),
            shape((own, cols), f32),
            shape((own, cols), f32),
        ),
        in_specs=[SMEM] + [ANY] * 9,
        out_specs=(VMEM,) * 5,
        scratch_shapes=[
            pltpu.VMEM((rows, kc), f32),
            pltpu.VMEM((rows, vc), f32),
            pltpu.VMEM((own, kc), f32),
            pltpu.VMEM((own, vc), f32),
            pltpu.VMEM((own, kc), f32),
            pltpu.VMEM((own, vc), f32),
            pltpu.SemaphoreType.DMA((9,)),
        ],
        cost_estimate=cost(4 * R * 2 * R * cols, 4 * d * R),
        compiler_params=limit(24),
        name="prep",
    )(core, *(in_hbm(x) for x in (basis_mine, basis_other, basis, mk, mv, fk, fv, sk, sv)))

    chunks = 8
    outs = tuple(shape(dims, f32) for dims in small)
    return pl.pallas_call(
        final_kernel,
        out_shape=outs[:4] + (shape((d, kc), bf16), shape((d, vc), bf16)) + outs[4:],
        in_specs=[VMEM] * 8 + [ANY],
        out_specs=(HBM,) * 10,
        scratch_shapes=[
            pltpu.VMEM((n_fs, 2 * own, cols), bf16),
            pltpu.VMEM((n_fs, rows, cols), bf16),
            pltpu.VMEM((d, kc), bf16),
            pltpu.VMEM((d, vc), bf16),
        ]
        + [pltpu.VMEM(dims, f32) for dims in small]
        + [
            pltpu.SemaphoreType.DMA,
            pltpu.SemaphoreType.DMA((chunks,)),
            pltpu.SemaphoreType.DMA((2, chunks)),
            pltpu.SemaphoreType.DMA((8,)),
        ],
        compiler_params=limit(32),
        name="update",
    )(squares, all_low, own_low, *held, in_hbm(gathered))


def solution(mesh):
    names = (*FS, *TP)
    torus = Mesh(mesh.devices.reshape(8, 8, 4, 2), names)
    split = P(FS, TP)
    in_specs = (P(FS, None), split, split, P(FS, None)) + (split,) * 6
    out_specs = (split,) * 4 + (P(None, TP),) * 2 + (split,) * 4
    return jax.shard_map(
        on_device, mesh=torus, in_specs=in_specs, out_specs=out_specs, check_vma=False
    )
```

```python
import jax
import jax.numpy as jnp
from jax import lax
from jax.experimental import pallas as pl
from jax.experimental.pallas import tpu as pltpu
from jax.sharding import Mesh
from jax.sharding import PartitionSpec as P

DK = 1024
DV = 2048
R = 256
FS = ("fs_0", "fs_1")
TP = ("tp_0", "tp_1")

learn_rate = 0.05
beta_first = 0.9
beta_second = 0.9
epsilon = 1e-08
norm_eps = 1e-06


f32 = jnp.float32
bf16 = jnp.bfloat16
VMEM = pl.BlockSpec(memory_space=pltpu.VMEM)
SMEM = pl.BlockSpec(memory_space=pltpu.SMEM)
ANY = pl.BlockSpec(memory_space=pl.ANY)
HBM = pl.BlockSpec(memory_space=pltpu.HBM)


def shape(dims, dtype):
    return jax.ShapeDtypeStruct(dims, dtype)


def cost(flops, moved):
    return pl.CostEstimate(flops=flops, bytes_accessed=moved, transcendentals=0)


def in_hbm(array):
    return pltpu.with_memory_space_constraint(array, pltpu.HBM)


def limit(mib):
    return pltpu.CompilerParams(vmem_limit_bytes=mib * 1024 * 1024)


def dot(a, b):
    return jnp.dot(a, b, preferred_element_type=f32)


def pack_kernel(core, mk, mv, fk, fv, sk, sv, basis, pack, copies):
    rows, kc = mk.shape
    half = copies.shape[2]
    mine = jnp.where(core[0] == 0, basis[:, :half].astype(f32), basis[:, half:].astype(f32))
    copies[...] = jnp.broadcast_to(mine.astype(bf16)[None], copies.shape)
    pack[:rows, :kc] = mk[...].astype(bf16)
    pack[:rows, kc:] = mv[...].astype(bf16)
    pack[rows:, :kc] = jnp.concatenate([fk[...], sk[...]], axis=0).astype(bf16)
    pack[rows:, kc:] = jnp.concatenate([fv[...], sv[...]], axis=0).astype(bf16)


def project_kernel(hi, lo, basis, out):
    b = basis[...]
    out[...] = (dot(hi[...], b) + dot(lo[...], b)).T


def project_both_kernel(core, hi, lo, basis, mine, out, kept, sem):
    half = mine.shape[0]
    keep = pltpu.make_async_copy(basis, kept, sem)
    keep.start()
    b = basis[...]
    at = pl.multiple_of(core[0] * half, half)
    other = pl.multiple_of((1 - core[0]) * half, half)
    out[pl.ds(at, half), :] = mine[...].astype(bf16)
    out[pl.ds(other, half), :] = (dot(hi[...], b) + dot(lo[...], b)).T.astype(bf16)
    keep.wait()


def squares_kernel(low, out):
    x = low[...].astype(f32)
    out[...] = jnp.broadcast_to(jnp.sum(x * x, keepdims=True)[None], out.shape)


def moments(low, scale, first, second):
    scaled = low * scale
    new_first = beta_first * first + (1.0 - beta_first) * scaled
    new_second = beta_second * second + (1.0 - beta_second) * scaled * scaled
    return new_first, new_second


def prep_kernel(
    core, mine, other, basis, mk, mv, fk, fv, sk, sv,
    full_basis, own_basis, master, first, second,
    mk_v, mv_v, fk_v, fv_v, sk_v, sv_v, sems,
):
    kc = mk.shape[1]
    half = mine.shape[1]
    at = pl.multiple_of(core[0] * half, half)
    at_other = pl.multiple_of((1 - core[0]) * half, half)
    loads = [
        pltpu.make_async_copy(mine, full_basis.at[:, pl.ds(at, half)], sems.at[0]),
        pltpu.make_async_copy(other, full_basis.at[:, pl.ds(at_other, half)], sems.at[1]),
        pltpu.make_async_copy(basis, own_basis, sems.at[2]),
        pltpu.make_async_copy(mk, mk_v, sems.at[3]),
        pltpu.make_async_copy(mv, mv_v, sems.at[4]),
        pltpu.make_async_copy(fk, fk_v, sems.at[5]),
        pltpu.make_async_copy(fv, fv_v, sems.at[6]),
        pltpu.make_async_copy(sk, sk_v, sems.at[7]),
        pltpu.make_async_copy(sv, sv_v, sems.at[8]),
    ]
    for load in loads:
        load.start()
    for load in loads:
        load.wait()
    master[:, :kc] = mk_v[...]
    master[:, kc:] = mv_v[...]
    first[:, :kc] = fk_v[...]
    first[:, kc:] = fv_v[...]
    second[:, :kc] = sk_v[...]
    second[:, kc:] = sv_v[...]


def final_kernel(
    squares, low, own_low, full_basis, basis, master, first, second, gathered,
    step_k, step_v, new_k, new_v, copy_k, copy_v, nf_k, ns_k, nf_v, ns_v,
    mom, masters, out_k, out_v,
    step_ks, step_vs, new_ks, new_vs, nf_ks, ns_ks, nf_vs, ns_vs, mom_sem, master_sem, out_sem, own_sem,
):
    n_fs, per, cols = mom.shape
    rows = master.shape[0]
    kc = step_k.shape[1]
    chunks = master_sem.shape[0]
    group = n_fs // chunks
    size = group * rows
    load = pltpu.make_async_copy(gathered.at[:, pl.ds(rows, per), :], mom, mom_sem)
    load.start()
    loads = []
    for k in range(chunks):
        at = pl.ds(k * group, group)
        source = gathered.at[at, pl.ds(0, rows), :]
        loads.append(pltpu.make_async_copy(source, masters.at[at], master_sem.at[k]))
        loads[k].start()

    stores = []

    def store(source, target, sem):
        stores.append(pltpu.make_async_copy(source, target, sem))
        stores[-1].start()

    total = jnp.sum(squares[...], axis=0)[:1, :1]
    scale = 1.0 / jnp.sqrt(total / (R * (DK + DV)) + norm_eps)
    nf, ns = moments(own_low[...], scale, first[...], second[...])
    nf_ks[...] = nf[:, :kc]
    nf_vs[...] = nf[:, kc:]
    ns_ks[...] = ns[:, :kc]
    ns_vs[...] = ns[:, kc:]

    own = per // 2
    i = lax.broadcasted_iota(jnp.int32, (n_fs * own, n_fs * per), 0)
    j = lax.broadcasted_iota(jnp.int32, (n_fs * own, n_fs * per), 1)
    at_first = (i // own) * per + i % own
    pick_first = jnp.where(j == at_first, 1.0, 0.0).astype(bf16)
    pick_second = jnp.where(j == at_first + own, 1.0, 0.0).astype(bf16)
    load.wait()
    both = mom[...].reshape(n_fs * per, cols)
    nf, ns = moments(low[...].astype(f32), scale, dot(pick_first, both), dot(pick_second, both))
    direction = (nf / (jnp.sqrt(ns) + epsilon)).astype(bf16)

    for k in range(chunks):
        at = pl.ds(k * size, size)
        step = dot(full_basis[at, :], direction)
        loads[k].wait()
        old = masters[pl.ds(k * group, group)].astype(f32).reshape(size, cols)
        copy = (old - learn_rate * step).astype(bf16)
        out_k[at, :] = copy[:, :kc]
        out_v[at, :] = copy[:, kc:]
        store(out_k.at[at], copy_k.at[at], out_sem.at[0, k])
        store(out_v.at[at], copy_v.at[at], out_sem.at[1, k])
        if k == 0:
            step = dot(basis[...], direction)
            step_ks[...] = step[:, :kc]
            step_vs[...] = step[:, kc:]
            new = master[...] - learn_rate * step
            new_ks[...] = new[:, :kc]
            new_vs[...] = new[:, kc:]
            sources = (step_ks, step_vs, new_ks, new_vs, nf_ks, ns_ks, nf_vs, ns_vs)
            targets = (step_k, step_v, new_k, new_v, nf_k, ns_k, nf_v, ns_v)
            for n in range(len(sources)):
                store(sources[n], targets[n], own_sem.at[n])
    for item in stores:
        item.wait()


def to_everyone(array, axis):
    copies = jnp.broadcast_to(array, (lax.axis_size(axis), *array.shape))
    return lax.all_to_all(copies, axis, split_axis=0, concat_axis=0, tiled=True)


def on_device(normed, key_cot, value_cot, basis, mk, mv, fk, sk, fv, sv):
    kc = key_cot.shape[1]
    cols = kc + value_cot.shape[1]
    rows = basis.shape[0]
    d = normed.shape[1]
    own = fk.shape[0]
    n_fs = lax.axis_size(FS)
    n_tp = lax.axis_size(TP)
    half = R // 2
    core = lax.axis_index("tp_1").astype(jnp.int32).reshape(1)
    per = rows + 2 * own
    pair = [(0, 1), (1, 0)]

    pack, copies = pl.pallas_call(
        pack_kernel,
        out_shape=(shape((per, cols), bf16), shape((n_fs, rows, half), bf16)),
        in_specs=[SMEM] + [VMEM] * 7,
        out_specs=(VMEM, VMEM),
        compiler_params=limit(24),
        name="pack",
    )(core, *(in_hbm(x) for x in (mk, mv, fk, fv, sk, sv, basis)))
    gathered = lax.all_gather(pack, FS, axis=0, tiled=True).reshape(n_fs, per, cols)
    basis_mine = lax.all_to_all(copies, FS, 0, 0, tiled=True).reshape(d, half)

    cot = jnp.concatenate([key_cot, value_cot], axis=1)
    grad = lax.dot_general(cot, normed, (((0,), (0,)), ((), ())), preferred_element_type=f32)
    hi = grad.astype(bf16)
    lo = (grad - hi.astype(f32)).astype(bf16)
    basis_mine, hi, lo = lax.optimization_barrier((basis_mine, hi, lo))
    basis_other = lax.ppermute(basis_mine, "tp_1", pair)
    project_cost = cost(4 * d * half * cols, 4 * d * cols + 2 * d * half)
    low_mine = pl.pallas_call(
        project_kernel,
        out_shape=shape((half, cols), f32),
        in_specs=[VMEM] * 3,
        out_specs=VMEM,
        cost_estimate=project_cost,
        compiler_params=limit(12),
        name="project_mine",
    )(hi, lo, basis_mine)
    parts, basis_other = pl.pallas_call(
        project_both_kernel,
        out_shape=(shape((R, cols), bf16), pltpu.HBM((d, half), bf16)),
        in_specs=[SMEM] + [VMEM] * 4,
        out_specs=(VMEM, HBM),
        scratch_shapes=[pltpu.SemaphoreType.DMA],
        cost_estimate=project_cost,
        compiler_params=limit(12),
        name="project_other",
    )(core, hi, lo, basis_other, low_mine)
    tiles = lax.all_to_all(parts.reshape(n_fs, own, cols), FS, 0, 0, tiled=True)
    own_low = jnp.sum(tiles.astype(f32), axis=0)

    all_low = to_everyone(own_low.astype(bf16), FS).reshape(R, cols)
    local = pl.pallas_call(
        squares_kernel,
        out_shape=shape((n_tp, 8, 128), f32),
        in_specs=[VMEM],
        out_specs=VMEM,
        compiler_params=limit(4),
        name="squares",
    )(all_low)
    squares = lax.all_to_all(local, TP, 0, 0, tiled=True)
    vc = cols - kc
    small = ((rows, kc), (rows, vc)) * 2 + ((own, kc), (own, kc), (own, vc), (own, vc))
    held = pl.pallas_call(
        prep_kernel,
        out_shape=(
            shape((d, R), bf16),
            shape((rows, R), bf16),
            shape((rows, cols), f32),
            shape((own, cols), f32),
            shape((own, cols), f32),
        ),
        in_specs=[SMEM] + [ANY] * 9,
        out_specs=(VMEM,) * 5,
        scratch_shapes=[
            pltpu.VMEM((rows, kc), f32),
            pltpu.VMEM((rows, vc), f32),
            pltpu.VMEM((own, kc), f32),
            pltpu.VMEM((own, vc), f32),
            pltpu.VMEM((own, kc), f32),
            pltpu.VMEM((own, vc), f32),
            pltpu.SemaphoreType.DMA((9,)),
        ],
        cost_estimate=cost(4 * R * 2 * R * cols, 4 * d * R),
        compiler_params=limit(24),
        name="prep",
    )(core, *(in_hbm(x) for x in (basis_mine, basis_other, basis, mk, mv, fk, fv, sk, sv)))

    chunks = 8
    outs = tuple(shape(dims, f32) for dims in small)
    return pl.pallas_call(
        final_kernel,
        out_shape=outs[:4] + (shape((d, kc), bf16), shape((d, vc), bf16)) + outs[4:],
        in_specs=[VMEM] * 8 + [ANY],
        out_specs=(HBM,) * 10,
        scratch_shapes=[
            pltpu.VMEM((n_fs, 2 * own, cols), bf16),
            pltpu.VMEM((n_fs, rows, cols), bf16),
            pltpu.VMEM((d, kc), bf16),
            pltpu.VMEM((d, vc), bf16),
        ]
        + [pltpu.VMEM(dims, f32) for dims in small]
        + [
            pltpu.SemaphoreType.DMA,
            pltpu.SemaphoreType.DMA((chunks,)),
            pltpu.SemaphoreType.DMA((2, chunks)),
            pltpu.SemaphoreType.DMA((8,)),
        ],
        compiler_params=limit(32),
        name="update",
    )(squares, all_low, own_low, *held, in_hbm(gathered))


def solution(mesh):
    names = (*FS, *TP)
    torus = Mesh(mesh.devices.reshape(8, 8, 4, 2), names)
    split = P(FS, TP)
    in_specs = (P(FS, None), split, split, P(FS, None)) + (split,) * 6
    out_specs = (split,) * 4 + (P(None, TP),) * 2 + (split,) * 4
    return jax.shard_map(
        on_device, mesh=torus, in_specs=in_specs, out_specs=out_specs, check_vma=False
    )
```

```python
import jax
import jax.numpy as jnp
from jax import lax
from jax.experimental import pallas as pl
from jax.experimental.pallas import tpu as pltpu
from jax.sharding import Mesh
from jax.sharding import PartitionSpec as P

DK = 1024
DV = 2048
R = 256
FS = ("fs_0", "fs_1")
TP = ("tp_0", "tp_1")

learn_rate = 0.05
beta_first = 0.9
beta_second = 0.9
epsilon = 1e-08
norm_eps = 1e-06


f32 = jnp.float32
bf16 = jnp.bfloat16
VMEM = pl.BlockSpec(memory_space=pltpu.VMEM)
SMEM = pl.BlockSpec(memory_space=pltpu.SMEM)
ANY = pl.BlockSpec(memory_space=pl.ANY)
HBM = pl.BlockSpec(memory_space=pltpu.HBM)


def shape(dims, dtype):
    return jax.ShapeDtypeStruct(dims, dtype)


def cost(flops, moved):
    return pl.CostEstimate(flops=flops, bytes_accessed=moved, transcendentals=0)


def in_hbm(array):
    return pltpu.with_memory_space_constraint(array, pltpu.HBM)


def limit(mib):
    return pltpu.CompilerParams(vmem_limit_bytes=mib * 1024 * 1024)


def dot(a, b):
    return jnp.dot(a, b, preferred_element_type=f32)


def pack_kernel(core, mk, mv, fk, fv, sk, sv, basis, pack, copies):
    rows, kc = mk.shape
    half = copies.shape[2]
    mine = jnp.where(core[0] == 0, basis[:, :half].astype(f32), basis[:, half:].astype(f32))
    copies[...] = jnp.broadcast_to(mine.astype(bf16)[None], copies.shape)
    pack[:rows, :kc] = mk[...].astype(bf16)
    pack[:rows, kc:] = mv[...].astype(bf16)
    pack[rows:, :kc] = jnp.concatenate([fk[...], sk[...]], axis=0).astype(bf16)
    pack[rows:, kc:] = jnp.concatenate([fv[...], sv[...]], axis=0).astype(bf16)


def project_kernel(hi, lo, basis, out):
    b = basis[...]
    out[...] = (dot(hi[...], b) + dot(lo[...], b)).T


def project_both_kernel(core, hi, lo, basis, mine, out, kept, sem):
    half = mine.shape[0]
    keep = pltpu.make_async_copy(basis, kept, sem)
    keep.start()
    b = basis[...]
    at = pl.multiple_of(core[0] * half, half)
    other = pl.multiple_of((1 - core[0]) * half, half)
    out[pl.ds(at, half), :] = mine[...]
    out[pl.ds(other, half), :] = (dot(hi[...], b) + dot(lo[...], b)).T
    keep.wait()


def squares_kernel(low, out):
    x = low[...].astype(f32)
    out[...] = jnp.broadcast_to(jnp.sum(x * x, keepdims=True)[None], out.shape)


def moments(low, scale, first, second):
    scaled = low * scale
    new_first = beta_first * first + (1.0 - beta_first) * scaled
    new_second = beta_second * second + (1.0 - beta_second) * scaled * scaled
    return new_first, new_second


def prep_kernel(
    core, mine, other, basis, mk, mv, fk, fv, sk, sv,
    full_basis, own_basis, master, first, second,
    mk_v, mv_v, fk_v, fv_v, sk_v, sv_v, sems,
):
    kc = mk.shape[1]
    half = mine.shape[1]
    at = pl.multiple_of(core[0] * half, half)
    at_other = pl.multiple_of((1 - core[0]) * half, half)
    loads = [
        pltpu.make_async_copy(mine, full_basis.at[:, pl.ds(at, half)], sems.at[0]),
        pltpu.make_async_copy(other, full_basis.at[:, pl.ds(at_other, half)], sems.at[1]),
        pltpu.make_async_copy(basis, own_basis, sems.at[2]),
        pltpu.make_async_copy(mk, mk_v, sems.at[3]),
        pltpu.make_async_copy(mv, mv_v, sems.at[4]),
        pltpu.make_async_copy(fk, fk_v, sems.at[5]),
        pltpu.make_async_copy(fv, fv_v, sems.at[6]),
        pltpu.make_async_copy(sk, sk_v, sems.at[7]),
        pltpu.make_async_copy(sv, sv_v, sems.at[8]),
    ]
    for load in loads:
        load.start()
    for load in loads:
        load.wait()
    master[:, :kc] = mk_v[...]
    master[:, kc:] = mv_v[...]
    first[:, :kc] = fk_v[...]
    first[:, kc:] = fv_v[...]
    second[:, :kc] = sk_v[...]
    second[:, kc:] = sv_v[...]


def final_kernel(
    squares, low, own_low, full_basis, basis, master, first, second, gathered,
    step_k, step_v, new_k, new_v, copy_k, copy_v, nf_k, ns_k, nf_v, ns_v,
    held, out_k, out_v,
    step_ks, step_vs, new_ks, new_vs, nf_ks, ns_ks, nf_vs, ns_vs, in_sem, out_sem, own_sem,
):
    n_fs, block, cols = held.shape
    rows = master.shape[0]
    per = block - rows
    kc = step_k.shape[1]
    chunks = in_sem.shape[0]
    group = n_fs // chunks
    size = group * rows
    loads = []
    for k in range(chunks):
        at = pl.ds(k * group, group)
        loads.append(pltpu.make_async_copy(gathered.at[at], held.at[at], in_sem.at[k]))
        loads[k].start()

    stores = []

    def store(source, target, sem):
        stores.append(pltpu.make_async_copy(source, target, sem))
        stores[-1].start()

    total = jnp.sum(squares[...], axis=0)[:1, :1]
    scale = 1.0 / jnp.sqrt(total / (R * (DK + DV)) + norm_eps)
    nf, ns = moments(own_low[...], scale, first[...], second[...])
    nf_ks[...] = nf[:, :kc]
    nf_vs[...] = nf[:, kc:]
    ns_ks[...] = ns[:, :kc]
    ns_vs[...] = ns[:, kc:]

    own = per // 2
    i = lax.broadcasted_iota(jnp.int32, (n_fs * own, n_fs * per), 0)
    j = lax.broadcasted_iota(jnp.int32, (n_fs * own, n_fs * per), 1)
    at_first = (i // own) * per + i % own
    pick_first = jnp.where(j == at_first, 1.0, 0.0).astype(bf16)
    pick_second = jnp.where(j == at_first + own, 1.0, 0.0).astype(bf16)
    for load in loads:
        load.wait()
    both = held[:, rows:].reshape(n_fs * per, cols)
    nf, ns = moments(low[...].astype(f32), scale, dot(pick_first, both), dot(pick_second, both))
    direction = (nf / (jnp.sqrt(ns) + epsilon)).astype(bf16)

    for k in range(chunks):
        at = pl.ds(k * size, size)
        step = dot(full_basis[at, :], direction)
        old = held[pl.ds(k * group, group), :rows].astype(f32).reshape(size, cols)
        copy = (old - learn_rate * step).astype(bf16)
        out_k[at, :] = copy[:, :kc]
        out_v[at, :] = copy[:, kc:]
        store(out_k.at[at], copy_k.at[at], out_sem.at[0, k])
        store(out_v.at[at], copy_v.at[at], out_sem.at[1, k])
        if k == 0:
            step = dot(basis[...], direction)
            step_ks[...] = step[:, :kc]
            step_vs[...] = step[:, kc:]
            new = master[...] - learn_rate * step
            new_ks[...] = new[:, :kc]
            new_vs[...] = new[:, kc:]
            sources = (step_ks, step_vs, new_ks, new_vs, nf_ks, ns_ks, nf_vs, ns_vs)
            targets = (step_k, step_v, new_k, new_v, nf_k, ns_k, nf_v, ns_v)
            for n in range(len(sources)):
                store(sources[n], targets[n], own_sem.at[n])
    for item in stores:
        item.wait()


def to_everyone(array, axis):
    copies = jnp.broadcast_to(array, (lax.axis_size(axis), *array.shape))
    return lax.all_to_all(copies, axis, split_axis=0, concat_axis=0, tiled=True)


def on_device(normed, key_cot, value_cot, basis, mk, mv, fk, sk, fv, sv):
    kc = key_cot.shape[1]
    cols = kc + value_cot.shape[1]
    rows = basis.shape[0]
    d = normed.shape[1]
    own = fk.shape[0]
    n_fs = lax.axis_size(FS)
    n_tp = lax.axis_size(TP)
    half = R // 2
    core = lax.axis_index("tp_1").astype(jnp.int32).reshape(1)
    per = rows + 2 * own
    pair = [(0, 1), (1, 0)]

    pack, copies = pl.pallas_call(
        pack_kernel,
        out_shape=(shape((per, cols), bf16), shape((n_fs, rows, half), bf16)),
        in_specs=[SMEM] + [VMEM] * 7,
        out_specs=(VMEM, VMEM),
        compiler_params=limit(24),
        name="pack",
    )(core, *(in_hbm(x) for x in (mk, mv, fk, fv, sk, sv, basis)))
    gathered = lax.all_gather(pack, FS, axis=0, tiled=True).reshape(n_fs, per, cols)
    basis_mine = lax.all_to_all(copies, FS, 0, 0, tiled=True).reshape(d, half)

    cot = jnp.concatenate([key_cot, value_cot], axis=1)
    grad = lax.dot_general(cot, normed, (((0,), (0,)), ((), ())), preferred_element_type=f32)
    hi = grad.astype(bf16)
    lo = (grad - hi.astype(f32)).astype(bf16)
    basis_mine, hi, lo = lax.optimization_barrier((basis_mine, hi, lo))
    basis_other = lax.ppermute(basis_mine, "tp_1", pair)
    project_cost = cost(4 * d * half * cols, 4 * d * cols + 2 * d * half)
    low_mine = pl.pallas_call(
        project_kernel,
        out_shape=shape((half, cols), f32),
        in_specs=[VMEM] * 3,
        out_specs=VMEM,
        cost_estimate=project_cost,
        compiler_params=limit(12),
        name="project_mine",
    )(hi, lo, basis_mine)
    parts, basis_other = pl.pallas_call(
        project_both_kernel,
        out_shape=(shape((R, cols), f32), pltpu.HBM((d, half), bf16)),
        in_specs=[SMEM] + [VMEM] * 4,
        out_specs=(VMEM, HBM),
        scratch_shapes=[pltpu.SemaphoreType.DMA],
        cost_estimate=project_cost,
        compiler_params=limit(12),
        name="project_other",
    )(core, hi, lo, basis_other, low_mine)
    tiles = lax.all_to_all(parts.reshape(n_fs, own, cols), FS, 0, 0, tiled=True)
    own_low = jnp.sum(tiles, axis=0)

    all_low = to_everyone(own_low.astype(bf16), FS).reshape(R, cols)
    local = pl.pallas_call(
        squares_kernel,
        out_shape=shape((n_tp, 8, 128), f32),
        in_specs=[VMEM],
        out_specs=VMEM,
        compiler_params=limit(4),
        name="squares",
    )(all_low)
    squares = lax.all_to_all(local, TP, 0, 0, tiled=True)
    vc = cols - kc
    small = ((rows, kc), (rows, vc)) * 2 + ((own, kc), (own, kc), (own, vc), (own, vc))
    held = pl.pallas_call(
        prep_kernel,
        out_shape=(
            shape((d, R), bf16),
            shape((rows, R), bf16),
            shape((rows, cols), f32),
            shape((own, cols), f32),
            shape((own, cols), f32),
        ),
        in_specs=[SMEM] + [ANY] * 9,
        out_specs=(VMEM,) * 5,
        scratch_shapes=[
            pltpu.VMEM((rows, kc), f32),
            pltpu.VMEM((rows, vc), f32),
            pltpu.VMEM((own, kc), f32),
            pltpu.VMEM((own, vc), f32),
            pltpu.VMEM((own, kc), f32),
            pltpu.VMEM((own, vc), f32),
            pltpu.SemaphoreType.DMA((9,)),
        ],
        cost_estimate=cost(4 * R * 2 * R * cols, 4 * d * R),
        compiler_params=limit(24),
        name="prep",
    )(core, *(in_hbm(x) for x in (basis_mine, basis_other, basis, mk, mv, fk, fv, sk, sv)))

    chunks = 2
    outs = tuple(shape(dims, f32) for dims in small)
    return pl.pallas_call(
        final_kernel,
        out_shape=outs[:4] + (shape((d, kc), bf16), shape((d, vc), bf16)) + outs[4:],
        in_specs=[VMEM] * 8 + [ANY],
        out_specs=(HBM,) * 10,
        scratch_shapes=[
            pltpu.VMEM((n_fs, per, cols), bf16),
            pltpu.VMEM((d, kc), bf16),
            pltpu.VMEM((d, vc), bf16),
        ]
        + [pltpu.VMEM(dims, f32) for dims in small]
        + [
            pltpu.SemaphoreType.DMA((chunks,)),
            pltpu.SemaphoreType.DMA((2, chunks)),
            pltpu.SemaphoreType.DMA((8,)),
        ],
        compiler_params=limit(32),
        name="update",
    )(squares, all_low, own_low, *held, in_hbm(gathered))


def solution(mesh):
    names = (*FS, *TP)
    torus = Mesh(mesh.devices.reshape(8, 8, 4, 2), names)
    split = P(FS, TP)
    in_specs = (P(FS, None), split, split, P(FS, None)) + (split,) * 6
    out_specs = (split,) * 4 + (P(None, TP),) * 2 + (split,) * 4
    return jax.shard_map(
        on_device, mesh=torus, in_specs=in_specs, out_specs=out_specs, check_vma=False
    )
```

```python
import jax
import jax.numpy as jnp
from jax import lax
from jax.experimental import pallas as pl
from jax.experimental.pallas import tpu as pltpu
from jax.sharding import Mesh
from jax.sharding import PartitionSpec as P

DK = 1024
DV = 2048
R = 256
FS = ("fs_0", "fs_1")
TP = ("tp_0", "tp_1")

learn_rate = 0.05
beta_first = 0.9
beta_second = 0.9
epsilon = 1e-08
norm_eps = 1e-06


f32 = jnp.float32
bf16 = jnp.bfloat16
VMEM = pl.BlockSpec(memory_space=pltpu.VMEM)
SMEM = pl.BlockSpec(memory_space=pltpu.SMEM)
ANY = pl.BlockSpec(memory_space=pl.ANY)
HBM = pl.BlockSpec(memory_space=pltpu.HBM)


def shape(dims, dtype):
    return jax.ShapeDtypeStruct(dims, dtype)


def cost(flops, moved):
    return pl.CostEstimate(flops=flops, bytes_accessed=moved, transcendentals=0)


def in_hbm(array):
    return pltpu.with_memory_space_constraint(array, pltpu.HBM)


def limit(mib):
    return pltpu.CompilerParams(vmem_limit_bytes=mib * 1024 * 1024)


def dot(a, b):
    return jnp.dot(a, b, preferred_element_type=f32)


def pack_kernel(core, mk, mv, fk, fv, sk, sv, basis, pack, copies):
    rows, kc = mk.shape
    half = copies.shape[2]
    mine = jnp.where(core[0] == 0, basis[:, :half].astype(f32), basis[:, half:].astype(f32))
    copies[...] = jnp.broadcast_to(mine.astype(bf16)[None], copies.shape)
    pack[:rows, :kc] = mk[...].astype(bf16)
    pack[:rows, kc:] = mv[...].astype(bf16)
    pack[rows:, :kc] = jnp.concatenate([fk[...], sk[...]], axis=0).astype(bf16)
    pack[rows:, kc:] = jnp.concatenate([fv[...], sv[...]], axis=0).astype(bf16)


def project_kernel(hi, lo, basis, out):
    b = basis[...]
    out[...] = (dot(hi[...], b) + dot(lo[...], b)).T


def project_both_kernel(core, hi, lo, basis, mine, out, kept, sem):
    half = mine.shape[0]
    keep = pltpu.make_async_copy(basis, kept, sem)
    keep.start()
    b = basis[...]
    at = pl.multiple_of(core[0] * half, half)
    other = pl.multiple_of((1 - core[0]) * half, half)
    out[pl.ds(at, half), :] = mine[...].astype(bf16)
    out[pl.ds(other, half), :] = (dot(hi[...], b) + dot(lo[...], b)).T.astype(bf16)
    keep.wait()


def squares_kernel(low, out):
    x = low[...].astype(f32)
    out[...] = jnp.broadcast_to(jnp.sum(x * x, keepdims=True)[None], out.shape)


def moments(low, scale, first, second):
    scaled = low * scale
    new_first = beta_first * first + (1.0 - beta_first) * scaled
    new_second = beta_second * second + (1.0 - beta_second) * scaled * scaled
    return new_first, new_second


def prep_kernel(
    core, mine, other, basis, mk, mv, fk, fv, sk, sv,
    full_basis, own_basis, master, first, second,
    mk_v, mv_v, fk_v, fv_v, sk_v, sv_v, sems,
):
    kc = mk.shape[1]
    half = mine.shape[1]
    at = pl.multiple_of(core[0] * half, half)
    at_other = pl.multiple_of((1 - core[0]) * half, half)
    loads = [
        pltpu.make_async_copy(mine, full_basis.at[:, pl.ds(at, half)], sems.at[0]),
        pltpu.make_async_copy(other, full_basis.at[:, pl.ds(at_other, half)], sems.at[1]),
        pltpu.make_async_copy(basis, own_basis, sems.at[2]),
        pltpu.make_async_copy(mk, mk_v, sems.at[3]),
        pltpu.make_async_copy(mv, mv_v, sems.at[4]),
        pltpu.make_async_copy(fk, fk_v, sems.at[5]),
        pltpu.make_async_copy(fv, fv_v, sems.at[6]),
        pltpu.make_async_copy(sk, sk_v, sems.at[7]),
        pltpu.make_async_copy(sv, sv_v, sems.at[8]),
    ]
    for load in loads:
        load.start()
    for load in loads:
        load.wait()
    master[:, :kc] = mk_v[...]
    master[:, kc:] = mv_v[...]
    first[:, :kc] = fk_v[...]
    first[:, kc:] = fv_v[...]
    second[:, :kc] = sk_v[...]
    second[:, kc:] = sv_v[...]


def final_kernel(
    squares, low, own_low, full_basis, basis, master, first, second, gathered,
    step_k, step_v, new_k, new_v, copy_k, copy_v, nf_k, ns_k, nf_v, ns_v,
    held, out_k, out_v,
    step_ks, step_vs, new_ks, new_vs, nf_ks, ns_ks, nf_vs, ns_vs, in_sem, out_sem, own_sem,
):
    n_fs, block, cols = held.shape
    rows = master.shape[0]
    per = block - rows
    kc = step_k.shape[1]
    chunks = in_sem.shape[0]
    group = n_fs // chunks
    size = group * rows
    loads = []
    for k in range(chunks):
        at = pl.ds(k * group, group)
        loads.append(pltpu.make_async_copy(gathered.at[at], held.at[at], in_sem.at[k]))
        loads[k].start()

    stores = []

    def store(source, target, sem):
        stores.append(pltpu.make_async_copy(source, target, sem))
        stores[-1].start()

    total = jnp.sum(squares[...], axis=0)[:1, :1]
    scale = 1.0 / jnp.sqrt(total / (R * (DK + DV)) + norm_eps)
    nf, ns = moments(own_low[...], scale, first[...], second[...])
    nf_ks[...] = nf[:, :kc]
    nf_vs[...] = nf[:, kc:]
    ns_ks[...] = ns[:, :kc]
    ns_vs[...] = ns[:, kc:]

    own = per // 2
    i = lax.broadcasted_iota(jnp.int32, (n_fs * own, n_fs * per), 0)
    j = lax.broadcasted_iota(jnp.int32, (n_fs * own, n_fs * per), 1)
    at_first = (i // own) * per + i % own
    pick_first = jnp.where(j == at_first, 1.0, 0.0).astype(bf16)
    pick_second = jnp.where(j == at_first + own, 1.0, 0.0).astype(bf16)
    for load in loads:
        load.wait()
    both = held[:, rows:].reshape(n_fs * per, cols)
    nf, ns = moments(low[...].astype(f32), scale, dot(pick_first, both), dot(pick_second, both))
    direction = (nf / (jnp.sqrt(ns) + epsilon)).astype(bf16)

    for k in range(chunks):
        at = pl.ds(k * size, size)
        step = dot(full_basis[at, :], direction)
        old = held[pl.ds(k * group, group), :rows].astype(f32).reshape(size, cols)
        copy = (old - learn_rate * step).astype(bf16)
        out_k[at, :] = copy[:, :kc]
        out_v[at, :] = copy[:, kc:]
        store(out_k.at[at], copy_k.at[at], out_sem.at[0, k])
        store(out_v.at[at], copy_v.at[at], out_sem.at[1, k])
        if k == 0:
            step = dot(basis[...], direction)
            step_ks[...] = step[:, :kc]
            step_vs[...] = step[:, kc:]
            new = master[...] - learn_rate * step
            new_ks[...] = new[:, :kc]
            new_vs[...] = new[:, kc:]
            sources = (step_ks, step_vs, new_ks, new_vs, nf_ks, ns_ks, nf_vs, ns_vs)
            targets = (step_k, step_v, new_k, new_v, nf_k, ns_k, nf_v, ns_v)
            for n in range(len(sources)):
                store(sources[n], targets[n], own_sem.at[n])
    for item in stores:
        item.wait()


def to_everyone(array, axis):
    copies = jnp.broadcast_to(array, (lax.axis_size(axis), *array.shape))
    return lax.all_to_all(copies, axis, split_axis=0, concat_axis=0, tiled=True)


def on_device(normed, key_cot, value_cot, basis, mk, mv, fk, sk, fv, sv):
    kc = key_cot.shape[1]
    cols = kc + value_cot.shape[1]
    rows = basis.shape[0]
    d = normed.shape[1]
    own = fk.shape[0]
    n_fs = lax.axis_size(FS)
    n_tp = lax.axis_size(TP)
    half = R // 2
    core = lax.axis_index("tp_1").astype(jnp.int32).reshape(1)
    per = rows + 2 * own
    pair = [(0, 1), (1, 0)]

    pack, copies = pl.pallas_call(
        pack_kernel,
        out_shape=(shape((per, cols), bf16), shape((n_fs, rows, half), bf16)),
        in_specs=[SMEM] + [VMEM] * 7,
        out_specs=(VMEM, VMEM),
        compiler_params=limit(24),
        name="pack",
    )(core, *(in_hbm(x) for x in (mk, mv, fk, fv, sk, sv, basis)))
    gathered = lax.all_gather(pack, FS, axis=0, tiled=True).reshape(n_fs, per, cols)
    basis_mine = lax.all_to_all(copies, FS, 0, 0, tiled=True).reshape(d, half)

    cot = jnp.concatenate([key_cot, value_cot], axis=1)
    grad = lax.dot_general(cot, normed, (((0,), (0,)), ((), ())), preferred_element_type=f32)
    hi = grad.astype(bf16)
    lo = (grad - hi.astype(f32)).astype(bf16)
    basis_mine, hi, lo = lax.optimization_barrier((basis_mine, hi, lo))
    basis_other = lax.ppermute(basis_mine, "tp_1", pair)
    project_cost = cost(4 * d * half * cols, 4 * d * cols + 2 * d * half)
    low_mine = pl.pallas_call(
        project_kernel,
        out_shape=shape((half, cols), f32),
        in_specs=[VMEM] * 3,
        out_specs=VMEM,
        cost_estimate=project_cost,
        compiler_params=limit(12),
        name="project_mine",
    )(hi, lo, basis_mine)
    parts, basis_other = pl.pallas_call(
        project_both_kernel,
        out_shape=(shape((R, cols), bf16), pltpu.HBM((d, half), bf16)),
        in_specs=[SMEM] + [VMEM] * 4,
        out_specs=(VMEM, HBM),
        scratch_shapes=[pltpu.SemaphoreType.DMA],
        cost_estimate=project_cost,
        compiler_params=limit(12),
        name="project_other",
    )(core, hi, lo, basis_other, low_mine)
    tiles = lax.all_to_all(parts.reshape(n_fs, own, cols), FS, 0, 0, tiled=True)
    own_low = jnp.sum(tiles.astype(f32), axis=0)

    all_low = to_everyone(own_low.astype(bf16), FS).reshape(R, cols)
    local = pl.pallas_call(
        squares_kernel,
        out_shape=shape((n_tp, 8, 128), f32),
        in_specs=[VMEM],
        out_specs=VMEM,
        compiler_params=limit(4),
        name="squares",
    )(all_low)
    squares = lax.all_to_all(local, TP, 0, 0, tiled=True)
    vc = cols - kc
    small = ((rows, kc), (rows, vc)) * 2 + ((own, kc), (own, kc), (own, vc), (own, vc))
    held = pl.pallas_call(
        prep_kernel,
        out_shape=(
            shape((d, R), bf16),
            shape((rows, R), bf16),
            shape((rows, cols), f32),
            shape((own, cols), f32),
            shape((own, cols), f32),
        ),
        in_specs=[SMEM] + [ANY] * 9,
        out_specs=(VMEM,) * 5,
        scratch_shapes=[
            pltpu.VMEM((rows, kc), f32),
            pltpu.VMEM((rows, vc), f32),
            pltpu.VMEM((own, kc), f32),
            pltpu.VMEM((own, vc), f32),
            pltpu.VMEM((own, kc), f32),
            pltpu.VMEM((own, vc), f32),
            pltpu.SemaphoreType.DMA((9,)),
        ],
        cost_estimate=cost(4 * R * 2 * R * cols, 4 * d * R),
        compiler_params=limit(24),
        name="prep",
    )(core, *(in_hbm(x) for x in (basis_mine, basis_other, basis, mk, mv, fk, fv, sk, sv)))

    chunks = 2
    outs = tuple(shape(dims, f32) for dims in small)
    return pl.pallas_call(
        final_kernel,
        out_shape=outs[:4] + (shape((d, kc), bf16), shape((d, vc), bf16)) + outs[4:],
        in_specs=[VMEM] * 8 + [ANY],
        out_specs=(HBM,) * 10,
        scratch_shapes=[
            pltpu.VMEM((n_fs, per, cols), bf16),
            pltpu.VMEM((d, kc), bf16),
            pltpu.VMEM((d, vc), bf16),
        ]
        + [pltpu.VMEM(dims, f32) for dims in small]
        + [
            pltpu.SemaphoreType.DMA((chunks,)),
            pltpu.SemaphoreType.DMA((2, chunks)),
            pltpu.SemaphoreType.DMA((8,)),
        ],
        compiler_params=limit(32),
        name="update",
    )(squares, all_low, own_low, *held, in_hbm(gathered))


def solution(mesh):
    names = (*FS, *TP)
    torus = Mesh(mesh.devices.reshape(8, 8, 4, 2), names)
    split = P(FS, TP)
    in_specs = (P(FS, None), split, split, P(FS, None)) + (split,) * 6
    out_specs = (split,) * 4 + (P(None, TP),) * 2 + (split,) * 4
    return jax.shard_map(
        on_device, mesh=torus, in_specs=in_specs, out_specs=out_specs, check_vma=False
    )
```
